32 devices in a mesh: ep: 4 (over y, x), tp: 8 (over z, core).
Axes of the slice: x: 2, y: 2, z: 4, core: 2. Of those that a mesh axis runs over, the one named last changes fastest.
Arguments:
- queries: bfloat16 [16, 64, 2, 512], P('tp', None, None, 'ep'), may hold values from -24 to 24
- key_vectors: bfloat16 [16, 64, 2, 512], P('tp', None, None, 'ep'), may hold values from -24 to 24
- value_vectors: bfloat16 [16, 64, 2, 512], P('tp', None, None, 'ep'), may hold values from -6 to 6
- mixer_weight: bfloat16 [1024, 2048], replicated, may hold values from -0.375 to 0.375
- expert_rows: bfloat16 [512, 2048], P('ep'), may hold values from -6 to 6
- norm_gain: float32 [2048], replicated, may hold values from 0.1 to 1.9
- route_ids: int32 [512, 2], P('ep'), may hold values from 0 to 7, all different within a row; in each aligned block of 128 rows (0 to 127, 128 to 255, ...) at most 64 rows name the same one
- route_logits: float32 [512, 2], P('ep'), may hold values from -4 to 4
- gate_weight: bfloat16 [8, 2048, 4096], P('ep', None, 'tp'), may hold values from -0.39648438 to 0.39648438
- up_weight: bfloat16 [8, 2048, 4096], P('ep', None, 'tp'), may hold values from -0.39648438 to 0.39648438
- down_weight: bfloat16 [8, 4096, 2048], P('ep', 'tp'), may hold values from -0.028076172 to 0.028076172
Outputs:
- mixer_out: bfloat16 [2, 512, 2048], P(None, ('ep', 'tp'))
- routed_out: bfloat16 [2048, 512], P('tp', 'ep')
The draws below stay inside these ranges and needn't reach their ends.
Inputs may be any that keep to these rules, and one draw needn't show every extreme that they name: `route_ids`: each row names 2 different experts. Among the 128 rows of one index of ep no expert is named more than 64 times, a bound that some expert reaches in such a block.
All inputs are finite; a program needn't handle non-finite values.
Results may differ from the reference program's by a relative error of at most 0.018.
Values may be sent and summed in bfloat16 or wider, within the bound.
A program may use at most 64 MiB of HBM per device.

```python
import math
import jax
import jax.numpy as jnp
import numpy as np
from jax import lax

D = 2048
HEADS = 16
HD = 64
FF = 4096
TOP = 2
SEQS = 2
SEG = 128
B_EP = 128
EXPERTS = 8
FF_DEV = 512
CAP = 64
LEN = 512
TOKENS_B = 512
N_EP = 4
N_TP = 8


def head_axes(key):
    direction = jax.random.normal(jax.random.fold_in(key, 101), (HEADS, HD), jnp.float32)
    return direction / jnp.sqrt(jnp.sum(direction * direction, axis=1, keepdims=True))


def noise_draw(key, array_shape):
    return jnp.clip(jax.random.normal(key, array_shape, jnp.float32), -4.0, 4.0)


def draw_queries(key, part):
    direction = head_axes(key)
    noise_part = noise_draw(jax.random.fold_in(key, 1), (HEADS, HD, SEQS, LEN))
    return (math.sqrt(HD) * direction[:, :, None, None] + noise_part).astype(jnp.bfloat16)


def draw_key_vectors(key, part):
    direction = head_axes(key)
    slow_rate = math.log(LEN) + 3.0
    fast_heads = jax.random.randint(jax.random.fold_in(key, 103), (HEADS,), 0, 2)
    reference_level = jnp.where(fast_heads > 0, 5.0, slow_rate).astype(jnp.float32)
    noise_perturbation = jax.random.uniform(jax.random.fold_in(key, 105), (HEADS, SEQS, LEN // SEG), jnp.float32, -0.7, 0.7)
    noise_perturbation = jnp.repeat(noise_perturbation, SEG, axis=2)
    element_locations = jax.random.randint(jax.random.fold_in(key, 107), (HEADS, SEQS, 3), 0, LEN)
    target_slot_numbers = jnp.arange(LEN, dtype=jnp.int32)
    spike_location = jnp.any(target_slot_numbers[None, None, :, None] == element_locations[:, :, None, :], axis=3)
    lookup_occurrence = jnp.where(spike_location, 0.5, reference_level[:, None, None] + noise_perturbation)
    noise_part = noise_draw(jax.random.fold_in(key, 2), (HEADS, HD, SEQS, LEN))
    return (noise_part - lookup_occurrence[:, None, :, :] * direction[:, :, None, None]).astype(jnp.bfloat16)


def raised(result, key, source, target, shards_of, factor):
    def block_of(dim):
        return (jnp.arange(result.shape[dim]) // (result.shape[dim] // shards_of)).reshape((-1,) + (1,) * (result.ndim - 1 - dim))

    one_side = jax.random.permutation(key, shards_of)[block_of(target)]
    second = (block_of(target) + shards_of // 2) % shards_of
    return jnp.where((block_of(source) == one_side) | (block_of(source) == second), factor * result, result)


def block_levels(stream_key, extent, cuts, smallest, top_value):
    level = 1.0
    for dim, blocks in cuts:
        draws = jax.random.uniform(jax.random.fold_in(jax.random.fold_in(stream_key, 6), dim), (blocks,), jnp.float32, smallest / len(cuts), top_value / len(cuts))
        level = level * jnp.repeat(jnp.exp(draws), extent[dim] // blocks).reshape((-1,) + (1,) * (len(extent) - 1 - dim))
    return level


def deal_out(own_key, own, number, rows, count, top, most, slope):
    order = jax.random.permutation(own_key, count)
    crowded, usual = portions_of(count, rows * top, most, slope, True), portions_of(count, rows * top, most, slope, False)
    places = jnp.arange(count)

    def named(sizes, rotation):
        used = int((sizes > 0).sum())
        fixed = max(1, used // 4)
        passed = fixed + (places - fixed + rotation * (used - fixed)) % max(1, count - fixed)
        return jnp.zeros((count,), jnp.int32).at[order[jnp.where(places < fixed, places, passed)]].set(jnp.asarray(sizes, jnp.int32))

    sizes = jnp.where(number % 4 == 0, named(crowded, number // 4), named(usual, number - number // 4 - 1))
    mixed = jax.random.permutation(jax.random.fold_in(own, 3), count)
    donor, taker = mixed[0:count // 2 * 2:2], mixed[1:count // 2 * 2:2]
    margin = jnp.minimum(sizes[donor] - 1, most - sizes[taker]) // 2
    margin = jnp.where((donor == order[0]) | (taker == order[0]) | (sizes[taker] == 0), 0, jnp.maximum(margin, 0))
    passed = jax.random.randint(jax.random.fold_in(own, 4), (count // 2,), 0, 1 << 20) % (margin + 1)
    sizes = sizes.at[donor].add(-passed).at[taker].add(passed)
    items = jnp.searchsorted(jnp.cumsum(sizes), jnp.arange(rows * top), side="right").astype(jnp.int32)
    table = items.reshape(top, rows).T
    table = table[jax.random.permutation(jax.random.fold_in(own, 1), rows)]
    rotation = jax.random.randint(jax.random.fold_in(own, 2), (rows, 1), 0, top)
    return jnp.take_along_axis(table, (jnp.arange(top)[None, :] + rotation) % top, axis=1)


def portions_of(number_of, total, most, slope, full):
    loads = [(1 << 20) // math.isqrt(grade ** slope) + 1 for grade in range(1, number_of + 1)]
    largest = most if full else min(most, max(-(-total // number_of), total * loads[0] // sum(loads)))
    least = 1 if total - largest >= number_of - 1 else 0
    given, rest = [largest] + [least] * (number_of - 1), total - largest - least * (number_of - 1)
    while rest > 0:
        movable = [i for i in range(1, number_of) if given[i] < largest] or [i for i in range(1, number_of) if given[i] < most]
        mass, left = sum([loads[i] for i in movable]), rest
        for i in movable:
            extra = min(most - given[i], max(1, left * loads[i] // mass), rest)
            given[i] = given[i] + extra
            rest = rest - extra
    return np.array(given)


def normal_values(key, extent, width, bound, split=(), held_as=jnp.bfloat16):
    result = jax.random.normal(key, extent, jnp.float32) * width
    if len(split) > 0:
        result = block_levels(key, extent, split, -0.22, 0.18) * result
    return jnp.clip(result, min=-bound, max=bound).astype(held_as)


def noise_with(stream_key, extent, width, most, cuts, heavy, kind=jnp.bfloat16):
    values = width * jax.random.normal(stream_key, extent, jnp.float32)
    if cuts:
        values = values * block_levels(stream_key, extent, cuts, -0.22, 0.18)
    return jnp.clip(raised(values, jax.random.fold_in(stream_key, 3), *heavy), -most, most).astype(kind)


def setup_inputs(seed: int = 0) -> dict:
    key_of = jax.random.split(jax.random.key(seed), 12)
    queries = draw_queries(jax.random.fold_in(key_of[11], 71), 0)
    key_vectors = draw_key_vectors(jax.random.fold_in(key_of[11], 71), 0)
    value_vectors = normal_values(key_of[2], (HEADS, HD, SEQS, LEN), 1.0, 6.0, ((0, 8), (3, 4)))
    mixer_weight = normal_values(key_of[3], (HEADS * HD, D), (HEADS * HD // 4) ** -0.5, 0.375)
    expert_rows = normal_values(key_of[4], (TOKENS_B, D), 1.0, 6.0, ((0, 4),))
    norm_gain = jnp.clip(1.0 + 0.18 * jax.random.normal(key_of[5], (D,), jnp.float32), 0.1, 1.9)
    route_ids_keys = jax.random.split(jax.random.fold_in(key_of[6], 1), TOKENS_B // B_EP)
    route_ids_turns = jax.random.permutation(jax.random.fold_in(key_of[6], 3), TOKENS_B // B_EP)
    route_ids = jax.vmap(lambda own, number: deal_out(jax.random.fold_in(key_of[6], 2), own, number, B_EP, EXPERTS, TOP, CAP, 2))(route_ids_keys, route_ids_turns).reshape((TOKENS_B, TOP))
    route_logits = normal_values(key_of[7], (TOKENS_B, TOP), 1.0, 4.0, ((0, 4),), jnp.float32)
    gate_weight = normal_values(key_of[8], (EXPERTS, D, FF), (3.0 * D ** -0.5), 0.39648438, ((0, 4), (2, 8)))
    up_weight = normal_values(key_of[9], (EXPERTS, D, FF), (3.0 * D ** -0.5), 0.39648438, ((0, 4), (2, 8)))
    down_weight = noise_with(key_of[10], (EXPERTS, FF, D), (0.3 * FF ** -0.5), 0.028076172, ((0, 4), (1, 8)), (1, 2, 8, 2.0))
    return {"queries": queries, "key_vectors": key_vectors, "value_vectors": value_vectors, "mixer_weight": mixer_weight, "expert_rows": expert_rows, "norm_gain": norm_gain, "route_ids": route_ids, "route_logits": route_logits, "gate_weight": gate_weight, "up_weight": up_weight, "down_weight": down_weight}


limit_value = 7.0
alpha_value = 1.702
norm_eps = 1e-06

def activate(gate_pre, up_pre):
    gate_clamped = jnp.minimum(gate_pre, limit_value)
    up_clamped = jnp.clip(up_pre, -limit_value, limit_value)
    return ((up_clamped + 1.0) * gate_clamped * jax.nn.sigmoid(alpha_value * gate_clamped)).astype(jnp.bfloat16)

def stick_block(query_part, key_part, value_part, query_start):
    scores = jnp.einsum('hdq,hdk->hqk', query_part.astype(jnp.float32), key_part.astype(jnp.float32)) * HD ** (-0.5)
    query_pos = query_start + lax.broadcasted_iota(jnp.int32, (SEG, LEN), 0)
    lookup_slot = lax.broadcasted_iota(jnp.int32, (SEG, LEN), 1)
    usable = (lookup_slot < query_pos)[None]
    log_keep = jnp.where(usable, jax.nn.log_sigmoid(-scores), 0.0)
    blocked = log_keep.reshape(HEADS, SEG, N_EP, SEG)
    within = lax.cumsum(blocked, axis=3, reverse=True) - blocked
    block_totals = lax.optimization_barrier(jnp.sum(blocked, axis=3))
    log_beta = jax.nn.log_sigmoid(scores).reshape(HEADS, SEG, N_EP, SEG)
    weight = jnp.where(usable.reshape(1, SEG, N_EP, SEG), jnp.exp(log_beta + within), 0.0).astype(jnp.bfloat16)
    block_values = jnp.einsum('hqbk,hdbk->hdqb', weight.astype(jnp.float32), value_part.reshape(HEADS, HD, N_EP, SEG).astype(jnp.float32))
    later_sums = lax.cumsum(block_totals, axis=2, reverse=True) - block_totals
    return lax.optimization_barrier(jnp.sum(jnp.exp(later_sums)[:, None] * block_values, axis=3)).astype(jnp.bfloat16)

def reference(queries, key_vectors, value_vectors, mixer_weight, expert_rows, norm_gain, route_ids, route_logits, gate_weight, up_weight, down_weight):

    def one_block(block_number):
        seq_index = block_number // N_EP
        query_start = (block_number % N_EP * SEG).astype(jnp.int32)
        query_seq = lax.dynamic_index_in_dim(queries, seq_index, 2, keepdims=False)
        query_part = lax.dynamic_slice_in_dim(query_seq, query_start, SEG, 2)
        key_part = lax.dynamic_index_in_dim(key_vectors, seq_index, 2, keepdims=False)
        value_part = lax.dynamic_index_in_dim(value_vectors, seq_index, 2, keepdims=False)
        return stick_block(query_part, key_part, value_part, query_start)
    attended = lax.map(one_block, jnp.arange(SEQS * N_EP, dtype=jnp.int32))
    attended = attended.reshape(SEQS, N_EP, HEADS, HD, SEG).transpose(0, 1, 4, 2, 3).reshape(SEQS, LEN, HEADS * HD)
    mixer_out = jnp.einsum('slc,cm->slm', attended.astype(jnp.float32), mixer_weight.astype(jnp.float32)).astype(jnp.bfloat16)
    values = expert_rows.astype(jnp.float32)
    scaled = values * lax.rsqrt(lax.optimization_barrier(jnp.mean(values * values, axis=-1, keepdims=True)) + norm_eps)
    normed = (scaled * norm_gain).astype(jnp.bfloat16)
    route_weight = jax.nn.softmax(route_logits, axis=-1)
    block_ids = route_ids.reshape(N_EP, B_EP * TOP)
    one_hot_matrix = (block_ids[:, :, None] == jnp.arange(EXPERTS, dtype=jnp.int32)[None, None, :]).astype(jnp.int32)
    earlier = jnp.cumsum(one_hot_matrix, axis=1) - one_hot_matrix
    slot_rank = lax.optimization_barrier(jnp.sum(earlier * one_hot_matrix, axis=2))
    source = jnp.arange(N_EP, dtype=jnp.int32)[:, None]
    token_index = source * B_EP + jnp.arange(B_EP * TOP, dtype=jnp.int32)[None, :] // TOP
    table_index = ((block_ids * N_EP + source) * CAP + slot_rank).reshape(-1).astype(jnp.int32)
    owner_token = jnp.zeros((EXPERTS * N_EP * CAP,), jnp.int32).at[table_index].set(token_index.reshape(-1))
    slot_rows = N_EP * CAP

    def one_expert(expert_index):
        owners = lax.dynamic_slice_in_dim(owner_token, expert_index * slot_rows, slot_rows)
        rows_in = normed[owners]
        gate_pre = jnp.dot(rows_in, lax.dynamic_index_in_dim(gate_weight, expert_index, 0, keepdims=False), preferred_element_type=jnp.float32)
        up_pre = jnp.dot(rows_in, lax.dynamic_index_in_dim(up_weight, expert_index, 0, keepdims=False), preferred_element_type=jnp.float32)
        hidden = activate(gate_pre, up_pre)
        down_part = lax.dynamic_index_in_dim(down_weight, expert_index, 0, keepdims=False)
        group_part = jnp.einsum('rgf,gfd->grd', hidden.reshape(slot_rows, N_TP, FF_DEV).astype(jnp.float32), down_part.reshape(N_TP, FF_DEV, D).astype(jnp.float32))
        rounded = lax.optimization_barrier(group_part.astype(jnp.bfloat16))
        return lax.optimization_barrier(jnp.sum(rounded.astype(jnp.float32), axis=0))
    expert_value = lax.map(one_expert, jnp.arange(EXPERTS, dtype=jnp.int32)).reshape(EXPERTS * slot_rows, D)
    picked = expert_value[table_index].reshape(TOKENS_B, TOP, D)
    combined = lax.optimization_barrier(jnp.sum(picked * route_weight[:, :, None], axis=1))
    routed_out = combined.T.astype(jnp.bfloat16)
    return (mixer_out, routed_out)
```

```python
import functools

import jax
import jax.numpy as jnp
from jax import lax
from jax.experimental import pallas as pl
from jax.experimental.pallas import tpu as pltpu
from jax.sharding import PartitionSpec as P

limit_value = 7.0
alpha_value = 1.702
norm_eps = 1e-06

MESH = pl.DeviceIdType.MESH
f32 = jnp.float32
bf16 = jnp.bfloat16
scope = jax.named_scope


def activate(gate_pre, up_pre):
    g = jnp.minimum(gate_pre, limit_value)
    u = jnp.clip(up_pre, -limit_value, limit_value)
    return ((u + 1.0) * g / (1.0 + jnp.exp(-alpha_value * g))).astype(bf16)


def partner_of(me, offset, count):
    other = me
    bit = 1
    while bit < count:
        set_bit = (offset // bit) % 2
        other = other + set_bit * bit * (1 - 2 * ((me // bit) % 2))
        bit *= 2
    return other


def split_sources(n_ep):
    near = [d for d in range(1, n_ep) if d & (d - 1) == 0][::-1]
    far = [d for d in range(1, n_ep) if d & (d - 1) != 0][::-1]
    return near, far


def kernel(
    n_ep,
    n_tp,
    q_hbm,
    k_hbm,
    v_hbm,
    x_hbm,
    gain_hbm,
    ids_hbm,
    logits_hbm,
    gate_hbm,
    up_hbm,
    down_hbm,
    mixer_hbm,
    mix_out,
    routed_out,
    q_ref,
    k_ref,
    v_ref,
    x_ref,
    gain_ref,
    ids_ref,
    logits_ref,
    wg,
    wu,
    wd,
    wm,
    xs,
    xr,
    wr,
    kvr,
    pb,
    cr,
    sb,
    rr,
    zb,
    zr,
    at_send,
    at_recv,
    qt_ref,
    kv_ref,
    wt_ref,
    wc,
    acc,
    tot,
    hs,
    ob,
    w_sem,
    in_sem,
    xf_ss,
    xf_rs,
    g_ss,
    g_rs,
    ff_ss,
    ff_rs,
    y_ss,
    y_rs,
    e_ss,
    e_rs,
    cf_rs,
    xn_ss,
    fn_ss,
    xn_rs,
    fn_rs,
    cn_rs,
    rn_rs,
    wt_rs,
    kv_ss,
    kv_rs,
    z_rs,
    a_rs,
    c0_rs,
    r_ss,
    c_ss,
    z_ss,
    a_ss,
    wt_ss,
):
    e = lax.axis_index("ep")
    t = lax.axis_index("tp")
    core = t % 2
    zi = t // 2
    zs = n_tp // 2
    mate = t + 1 - 2 * core
    heads, seqs, seg, hd = qt_ref.shape
    tokens, width = x_ref.shape
    half = tokens // 2
    quarter = tokens // 4
    zp = zi % 2
    zmate = t + 2 - 4 * zp
    slots = wt_ref.shape[1]
    local_experts = wg.shape[0]
    ch = width // n_tp
    pp = seg // n_tp
    near, distances = split_sources(n_ep)
    passes = len(near)
    count = len(distances)
    part = tokens // passes
    group = zs // 2
    everything = slice(None)

    weights = [
        pltpu.make_async_copy(src, dst, w_sem.at[i])
        for i, (src, dst) in enumerate(
            ((gate_hbm, wg), (up_hbm, wu), (down_hbm, wd), (mixer_hbm, wm))
        )
    ]
    inputs = [
        pltpu.make_async_copy(src, dst, in_sem.at[i])
        for i, (src, dst) in enumerate(
            (
                (x_hbm, x_ref),
                (q_hbm, q_ref),
                (k_hbm, k_ref),
                (v_hbm, v_ref),
                (ids_hbm, ids_ref),
                (logits_hbm, logits_ref),
                (gain_hbm, gain_ref),
            )
        )
    ]

    def ep_peer(d):
        return partner_of(e, d, n_ep)

    barrier = pltpu.get_barrier_semaphore()
    for d in range(1, n_ep):
        pl.semaphore_signal(barrier, inc=1, device_id={"ep": ep_peer(d)}, device_id_type=MESH)
    for d in range(1, n_tp):
        pl.semaphore_signal(
            barrier, inc=1, device_id={"tp": (t + d) % n_tp}, device_id_type=MESH
        )
    for copy in inputs:
        copy.start()

    def nth(i):
        return sum(jnp.where(i == n, d, 0) for n, d in enumerate(distances))

    def remote(src, dst, send, recv, axis, to):
        return pltpu.make_async_remote_copy(
            src_ref=src,
            dst_ref=dst,
            send_sem=send,
            recv_sem=recv,
            device_id={axis: to},
            device_id_type=MESH,
        )

    def settle_bytes(ref, sem):
        pltpu.make_async_copy(ref, ref, sem).wait()

    mine = pl.ds(pl.multiple_of(core * half, half), half)
    piece = pl.ds(pl.multiple_of(core * half + zp * quarter, quarter), quarter)

    def span(h):
        return pl.ds(pl.multiple_of(h * part, part), part)

    def own_part(h):
        return pl.ds(pl.multiple_of(h * part + core * (part // 2), part // 2), part // 2)

    def xf_copy(i):
        d = nth(i)
        return remote(xs.at[piece], xr.at[d, piece], xf_ss.at[i], xf_rs.at[i], "ep", ep_peer(d))

    def g_copy(i):
        ref = xr.at[nth(i), piece]
        return remote(ref, ref, g_ss.at[i], g_rs.at[i], "tp", zmate)

    def ff_copy(i):
        ref = xr.at[nth(i), mine]
        return remote(ref, ref, ff_ss.at[i], ff_rs.at[i], "tp", mate)

    def xn_copy(n, h):
        rows = own_part(h)
        return remote(
            xs.at[rows],
            xr.at[near[n], rows],
            xn_ss.at[n],
            xn_rs.at[n, h],
            "ep",
            ep_peer(near[n]),
        )

    def fn_copy(n, h):
        ref = xr.at[near[n], own_part(h)]
        return remote(ref, ref, fn_ss.at[n], fn_rs.at[n, h], "tp", mate)

    def wt_copy(d):
        return remote(
            wt_ref.at[ep_peer(d)], wr.at[d], wt_ss.at[0], wt_rs.at[d - 1], "ep", ep_peer(d)
        )

    def kv_copy(d):
        return remote(
            kv_ref, kvr.at[d], kv_ss.at[d - 1], kv_rs.at[d - 1], "ep", (e + d) % n_ep
        )

    def c_copy(d, c, rows, sem):
        return remote(
            pb.at[d, 1 - core, c, rows], cr.at[d, c, rows], c_ss.at[0], sem, "tp", mate
        )

    def r_copy(n, h, k):
        c = (zi + k) % zs
        return remote(
            sb.at[near[n], c, span(h)],
            rr.at[near[n], c, span(h)],
            r_ss.at[0],
            rn_rs.at[n, h, k - 1],
            "ep",
            ep_peer(near[n]),
        )

    def y_copy(i, k):
        d = nth(i)
        c = (zi + k) % zs
        return remote(sb.at[d, c], rr.at[d, k], y_ss.at[i], y_rs.at[i], "tp", c * 2 + core)

    def e_copy(i):
        d = nth(i)
        return remote(sb.at[d, zi], rr.at[d, 0], e_ss.at[i], e_rs.at[i], "ep", ep_peer(d))

    def z_copy(k, h):
        dz = (zi + k) % zs
        return remote(
            zb.at[dz, span(h)],
            zr.at[k, span(h)],
            z_ss.at[0],
            z_rs.at[0],
            "tp",
            dz * 2 + core,
        )

    def a_copy(d):
        to = (t + d) % n_tp
        return remote(at_send.at[to], at_recv.at[t], a_ss.at[0], a_rs.at[0], "tp", to)

    with scope("xload"):
        for copy in inputs:
            copy.wait()
    for copy in weights:
        copy.start()

    with scope("norm0"):
        values = x_ref[...].astype(f32)
        mean = jnp.mean(values * values, axis=-1, keepdims=True)
        xs[...] = (values * lax.rsqrt(mean + norm_eps) * gain_ref[...]).astype(bf16)

    top = ids_ref.shape[0]
    logits = [logits_ref[k : k + 1] for k in range(top)]
    peak = functools.reduce(jnp.maximum, logits)
    powers = [jnp.exp(value - peak) for value in logits]
    share = 1.0 / functools.reduce(jnp.add, powers)
    slot = lax.broadcasted_iota(jnp.int32, (slots, tokens), 0)
    for g in range(n_ep):
        expert = jnp.where(slot < local_experts, g * local_experts + slot, -1)
        table = jnp.zeros((slots, tokens), f32)
        for k in range(top):
            table = table + jnp.where(ids_ref[k : k + 1] == expert, powers[k] * share, 0.0)
        wt_ref[g] = table

    with scope("barrier"):
        pl.semaphore_wait(barrier, n_ep - 1 + n_tp - 1)
    for d in range(1, n_ep):
        wt_copy(d).start()
    for i in range(count):
        xf_copy(i).start()
    for h in range(passes):
        for n in range(passes):
            xn_copy(n, h).start()

    rows = hd * seqs
    for s in range(seqs):
        pick = (
            (
                lax.broadcasted_iota(jnp.int32, (hd, rows), 1)
                == lax.broadcasted_iota(jnp.int32, (hd, rows), 0) * seqs + s
            )
            .astype(f32)
            .astype(bf16)
        )
        for h in range(heads):
            kv_ref[0, h, s] = jnp.dot(pick, k_ref[h], preferred_element_type=f32).astype(bf16)
            kv_ref[1, h, s] = jnp.dot(pick, v_ref[h], preferred_element_type=f32).astype(bf16)
            query = jnp.dot(pick, q_ref[h], preferred_element_type=f32)
            qt_ref[h, s] = query.T.astype(bf16)

    def up(j, lhs):
        gate_pre = jnp.dot(lhs(), wg[j], preferred_element_type=f32)
        up_pre = jnp.dot(lhs(), wu[j], preferred_element_type=f32)
        hs[j] = activate(gate_pre, up_pre)

    def down(sources, columns, rows, sems):
        size = tokens // len(sources)
        for k in range(1, zs + 1):
            c = (zi + k) % zs
            for p in range(2):
                place = pl.ds(pl.multiple_of((2 * c + p) * ch, ch), ch)
                terms = [
                    jnp.dot(hs[j], wd[j, :, place], preferred_element_type=f32)
                    for j in range(local_experts)
                ]
                for n, d in enumerate(sources):
                    total = None
                    for j in range(local_experts):
                        term = columns[n][:, j : j + 1] * terms[j][n * size : (n + 1) * size]
                        total = term if total is None else total + term
                    pb[d, p, c, rows] = total.astype(bf16)
            if k % group == 0:
                for q in range(k - group + 1, k + 1):
                    for d in sources:
                        c_copy(d, (zi + q) % zs, rows, sems.at[k // group - 1]).start()

    def joined(d, c, rows):
        sb[d, c, rows] = (pb[d, core, c, rows].astype(f32) + cr[d, c, rows].astype(f32)).astype(
            bf16
        )

    def finish_own():
        for b in range(2):
            settle_bytes(cr.at[0, pl.ds(0, group)], c0_rs.at[b])
        for c in range(zs):
            joined(0, c, everything)

    def finish_far(i):
        d = nth(i)
        for b in range(2):
            settle_bytes(cr.at[d, pl.ds(0, group)], cf_rs.at[i, b])
            for k in range(b * group + 1, (b + 1) * group + 1):
                joined(d, (zi + k) % zs, everything)
                if k < zs:
                    y_copy(i, k).start()

    def finish_near(h):
        for b in range(2):
            settle_bytes(cr.at[pl.ds(0, passes), pl.ds(0, group), span(h)], cn_rs.at[h, b])
            for k in range(b * group + 1, (b + 1) * group + 1):
                for n in range(passes):
                    joined(near[n], (zi + k) % zs, span(h))
                    r_copy(n, h, k).start()

    def gathered(i):
        d = nth(i)
        settle_bytes(rr.at[d, pl.ds(0, zs - 1)], y_rs.at[i])
        total = sb[d, zi].astype(f32)
        for k in range(1, zs):
            total = total + rr[d, k].astype(f32)
        sb[d, zi] = total.astype(bf16)
        e_copy(i).start()

    def settle(h):
        for k in range(1, zs + 1):
            c = (zi + k) % zs
            own = sb[0, c, span(h)].astype(f32)
            for n in range(passes):
                r_copy(n, h, k).wait_recv()
                own = own + rr[near[n], c, span(h)].astype(f32)
            if k < zs:
                zb[c, span(h)] = own.astype(bf16)
                z_copy(k, h).start()
            else:
                ob[span(h)] = own

    pairs = heads * seqs
    tall = pairs * seg
    row_id = lax.broadcasted_iota(jnp.int32, (2 * seg, 2 * seg), 0) % seg
    col_id = lax.broadcasted_iota(jnp.int32, (2 * seg, 2 * seg), 1)
    later_mask = ((row_id > col_id) | (col_id >= seg)).astype(f32).astype(bf16)
    scale = hd ** (-0.5)

    def block(kv, diagonal):
        scores = jnp.concatenate(
            [
                jnp.dot(qt_ref[p // seqs, p % seqs], kv[0, p // seqs, p % seqs],
                        preferred_element_type=f32)
                for p in range(pairs)
            ],
            axis=0,
        ) * scale
        log_term = jnp.log(1.0 + jnp.exp(-jnp.abs(scores)))
        keep = -(jnp.maximum(scores, 0.0) + log_term)
        beta = jnp.minimum(scores, 0.0) - log_term
        if diagonal:
            usable = lax.broadcasted_iota(jnp.int32, (tall, seg), 1) < (
                lax.broadcasted_iota(jnp.int32, (tall, seg), 0) % seg
            )
            keep = jnp.where(usable, keep, 0.0)
        high = keep.astype(bf16)
        low = (keep - high.astype(f32)).astype(bf16)
        sums = jnp.dot(
            jnp.concatenate([high, low], axis=1), later_mask, preferred_element_type=f32
        )
        weight = jnp.exp(beta + sums[:, :seg])
        if diagonal:
            weight = jnp.where(usable, weight, 0.0)
        weight = weight.astype(bf16)
        out = jnp.concatenate(
            [
                lax.dot_general(
                    weight[p * seg : (p + 1) * seg],
                    kv[1, p // seqs, p % seqs],
                    (((1,), (1,)), ((), ())),
                    preferred_element_type=f32,
                )
                for p in range(pairs)
            ],
            axis=0,
        )
        return out, sums[:, seg : seg + hd]

    with scope("diag"):
        acc[...], tot[...] = block(kv_ref, True)

    with scope("waitfar"):
        for i in range(count):
            xf_copy(i).wait_recv()
            g_copy(i).start()
    with scope("weights"):
        for copy in weights[:3]:
            copy.wait()
    with scope("up0"):
        for j in range(local_experts):
            up(j, lambda: xs[...])
    with scope("down0"):
        down([0], [wt_ref[e].T], everything, c0_rs)
    for k in range(1, n_ep):

        @pl.when(e + k < n_ep)
        def _():
            kv_copy(k).start()

    def share_near(h):
        with scope("xwait"):
            for n in range(passes):
                xn_copy(n, h).wait_recv()
                fn_copy(n, h).start()

    def share_far(i):
        with scope("gwait"):
            g_copy(i).wait_recv()
            ff_copy(i).start()

    def near_pass(h, middle):
        with scope("fwait"):
            for n in range(passes):
                fn_copy(n, h).wait_recv()

        def lhs():
            return jnp.concatenate([xr[d, span(h)] for d in near], axis=0)

        for j in range(local_experts):
            with scope("up"):
                up(j, lhs)
            if j == 0:
                middle()
        with scope("down"):
            down(near, [wc[n, span(h)] for n in range(passes)], span(h), cn_rs.at[h])

    def far_pass(i, middle):
        d = nth(i)
        with scope("fwait"):
            ff_copy(i).wait_recv()
        for j in range(local_experts):
            with scope("up"):
                up(j, lambda: xr[d])
            if j == 0:
                middle()
        with scope("downfar"):
            wt_copy(d).wait_recv()
            down([d], [wr[d].T], everything, cf_rs.at[i])

    def first_passes(h, carry):
        share_near(h)

        def middle():
            with scope("finish"):

                @pl.when(h > 0)
                def _():
                    finish_near(h - 1)

                @pl.when(h == 0)
                def _():
                    finish_own()

            if distances:

                @pl.when(h == passes - 2)
                def _():
                    share_far(0)

        near_pass(h, middle)
        return carry

    def far_passes(i, carry):
        def middle():
            @pl.when(i == 0)
            def _():
                with scope("finish"):
                    finish_near(passes - 2)

            @pl.when(i > 0)
            def _():
                finish_far(i - 1)

            @pl.when(i < count - 1)
            def _():
                share_far(i + 1)

            @pl.when(i == count - 1)
            def _():
                share_near(passes - 1)

        far_pass(i, middle)
        return carry

    def last_middle():
        with scope("finishfar"):
            if distances:
                finish_far(count - 1)
            else:
                finish_own()

    for n in range(passes):
        wt_copy(near[n]).wait_recv()
        wc[n] = wr[near[n]].T
    lax.fori_loop(0, passes - 1, first_passes, 0)
    lax.fori_loop(0, count, far_passes, 0)
    if not distances:
        share_near(passes - 1)
    near_pass(passes - 1, last_middle)
    with scope("finlast"):
        finish_near(passes - 1)

    def further(d, carry):
        kv_copy(d).wait_recv()
        out, total = block(kvr.at[d], False)
        later = tot[...]
        acc[...] = acc[...] + jnp.exp(later) * out
        tot[...] = later + total
        return carry

    with scope("further"):
        lax.fori_loop(1, e + 1, further, 0)
    with scope("asend"):
        for p in range(pairs):
            h, s = p // seqs, p % seqs
            for c in range(n_tp):
                at_send[c, s * pp : (s + 1) * pp, h * hd : (h + 1) * hd] = acc[
                    p * seg + c * pp : p * seg + (c + 1) * pp
                ].astype(bf16)
        for d in range(1, n_tp):
            a_copy(d).start()
        at_recv[t] = at_send[t]

    for h in range(passes):
        if h == passes - 1:
            with scope("gathered"):
                lax.fori_loop(0, count, lambda i, carry: (gathered(i), carry)[1], 0)
        with scope("settle"):
            settle(h)

    with scope("wmix"):
        weights[3].wait()
    with scope("await"):
        settle_bytes(at_recv.at[pl.ds(0, n_tp - 1)], a_rs.at[0])
    with scope("mix"):
        wide = jnp.concatenate([at_recv[c] for c in range(n_tp)], axis=1)
        mixed = jnp.dot(wide, wm[...], preferred_element_type=f32)
        for s in range(seqs):
            mix_out[s] = mixed[s * pp : (s + 1) * pp].astype(bf16)

    with scope("zfin"):
        total = ob[...]
        settle_bytes(zr.at[pl.ds(0, zs - 1)], z_rs.at[0])
        for k in range(1, zs):
            total = total + zr[k].astype(f32)
        for i, d in enumerate(distances):
            e_copy(i).wait_recv()
            total = total + rr[d, 0].astype(f32)
        routed_out[...] = total.T.astype(bf16)

    with scope("drain"):
        settle_bytes(wt_ref.at[pl.ds(0, n_ep - 1)], wt_ss.at[0])
        for i in range(count):
            xf_copy(i).wait_send()
            g_copy(i).wait_send()
            ff_copy(i).wait_send()
            settle_bytes(sb.at[0, pl.ds(0, zs - 1)], y_ss.at[i])
            e_copy(i).wait_send()
        for n in range(passes):
            settle_bytes(xs.at[mine], xn_ss.at[n])
            settle_bytes(xs.at[mine], fn_ss.at[n])
        settle_bytes(cr, c_ss.at[0])
        settle_bytes(sb.at[pl.ds(0, passes)], r_ss.at[0])
        settle_bytes(zb.at[pl.ds(0, zs - 1)], z_ss.at[0])
        settle_bytes(at_send.at[pl.ds(0, n_tp - 1)], a_ss.at[0])
        for k in range(1, n_ep):

            @pl.when(e + k < n_ep)
            def _():
                kv_copy(k).wait_send()


def hand_over(mixed_ref, routed_ref, mix_out, routed_out, sems):
    copies = [
        pltpu.make_async_copy(src, dst, sems.at[i])
        for i, (src, dst) in enumerate(((mixed_ref, mix_out), (routed_ref, routed_out)))
    ]
    for copy in copies:
        copy.start()
    for copy in copies:
        copy.wait()


def body(
    queries,
    key_vectors,
    value_vectors,
    mixer_weight,
    expert_rows,
    norm_gain,
    route_ids,
    route_logits,
    gate_weight,
    up_weight,
    down_weight,
):
    n_ep, n_tp = lax.axis_size("ep"), lax.axis_size("tp")
    heads, hd, seqs, seg = queries.shape
    tokens, width = expert_rows.shape
    local_experts, _, ff = gate_weight.shape
    zs, ch, pp = n_tp // 2, width // n_tp, seg // n_tp

    top = route_ids.shape[1]
    slots = 8 * -(-local_experts // 8)
    pairs = heads * seqs
    near, distances = split_sources(n_ep)
    passes, count = len(near), max(len(distances), 1)
    kv_shape = (2, heads, seqs, hd, seg)

    def merged(rows):
        return rows.reshape(heads, hd * seqs, seg)

    vmem = pl.BlockSpec(memory_space=pltpu.VMEM)
    anywhere = pl.BlockSpec(memory_space=pltpu.HBM)
    dma = pltpu.SemaphoreType.DMA
    outs = 2 * seqs * pp * width + 2 * ch * tokens
    limit = (60 * 1024 * 1024) - outs - (64 << 10)
    shapes = ((seqs, pp, width), (ch, tokens))
    results = pl.pallas_call(
        functools.partial(kernel, n_ep, n_tp),
        out_shape=tuple(pltpu.VMEM(shape, bf16) for shape in shapes),
        in_specs=[anywhere] * 11,
        out_specs=(vmem, vmem),
        scratch_shapes=[
            pltpu.VMEM((heads, hd * seqs, seg), bf16),
            pltpu.VMEM((heads, hd * seqs, seg), bf16),
            pltpu.VMEM((heads, hd * seqs, seg), bf16),
            pltpu.VMEM((tokens, width), bf16),
            pltpu.VMEM((1, width), f32),
            pltpu.VMEM((top, tokens), jnp.int32),
            pltpu.VMEM((top, tokens), f32),
            pltpu.VMEM(gate_weight.shape, bf16),
            pltpu.VMEM(up_weight.shape, bf16),
            pltpu.VMEM(down_weight.shape, bf16),
            pltpu.VMEM(mixer_weight.shape, bf16),
            pltpu.VMEM((tokens, width), bf16),
            pltpu.VMEM((n_ep, tokens, width), bf16),
            pltpu.VMEM((n_ep, slots, tokens), f32),
            pltpu.VMEM((n_ep,) + kv_shape, bf16),
            pltpu.VMEM((n_ep, 2, zs, tokens, ch), bf16),
            pltpu.VMEM((n_ep, zs, tokens, ch), bf16),
            pltpu.VMEM((n_ep, zs, tokens, ch), bf16),
            pltpu.VMEM((n_ep, zs, tokens, ch), bf16),
            pltpu.VMEM((zs, tokens, ch), bf16),
            pltpu.VMEM((zs, tokens, ch), bf16),
            pltpu.VMEM((n_tp, seqs * pp, heads * hd), bf16),
            pltpu.VMEM((n_tp, seqs * pp, heads * hd), bf16),
            pltpu.VMEM((heads, seqs, seg, hd), bf16),
            pltpu.VMEM(kv_shape, bf16),
            pltpu.VMEM((n_ep, slots, tokens), f32),
            pltpu.VMEM((passes, tokens, slots), f32),
            pltpu.VMEM((pairs * seg, hd), f32),
            pltpu.VMEM((pairs * seg, hd), f32),
            pltpu.VMEM((local_experts, tokens, ff), bf16),
            pltpu.VMEM((tokens, ch), f32),
            dma((4,)),
            dma((7,)),
        ]
        + [dma((count,))] * 10
        + [dma((count, 2))]
        + [dma((passes,))] * 2
        + [dma((passes, passes))] * 2
        + [dma((passes, 2)), dma((passes, passes, zs))]
        + [dma((n_ep - 1,))] * 3
        + [dma((1,))] * 2
        + [dma((2,))]
        + [dma((1,))] * 5,
        compiler_params=pltpu.CompilerParams(
            collective_id=0, has_side_effects=True, vmem_limit_bytes=limit
        ),
    )(
        merged(queries),
        merged(key_vectors),
        merged(value_vectors),
        expert_rows,
        norm_gain[None, :],
        route_ids.T,
        route_logits.T,
        gate_weight,
        up_weight,
        down_weight,
        mixer_weight,
    )
    return pl.pallas_call(
        hand_over,
        out_shape=tuple(jax.ShapeDtypeStruct(shape, bf16) for shape in shapes),
        in_specs=[vmem] * 2,
        out_specs=(anywhere, anywhere),
        scratch_shapes=[dma((2,))],
        compiler_params=pltpu.CompilerParams(vmem_limit_bytes=1 << 20),
    )(*results)


def solution(mesh):
    in_specs = (
        P("tp", None, None, "ep"),
        P("tp", None, None, "ep"),
        P("tp", None, None, "ep"),
        P(),
        P("ep", None),
        P(),
        P("ep", None),
        P("ep", None),
        P("ep", None, "tp"),
        P("ep", None, "tp"),
        P("ep", "tp", None),
    )
    out_specs = (P(None, ("ep", "tp"), None), P("tp", "ep"))
    return jax.shard_map(body, mesh=mesh, in_specs=in_specs, out_specs=out_specs, check_vma=False)
```

```python
import functools

import jax
import jax.numpy as jnp
from jax import lax
from jax.experimental import pallas as pl
from jax.experimental.pallas import tpu as pltpu
from jax.sharding import PartitionSpec as P

limit_value = 7.0
alpha_value = 1.702
norm_eps = 1e-06

MESH = pl.DeviceIdType.MESH
f32 = jnp.float32
bf16 = jnp.bfloat16
scope = jax.named_scope


def activate(gate_pre, up_pre, weight):
    g = jnp.minimum(gate_pre, limit_value)
    u = jnp.clip(up_pre, -limit_value, limit_value)
    sigmoid2 = 1.0 + jnp.tanh((0.5 * alpha_value) * g)
    return ((u + 1.0) * (g * (0.5 * weight)) * sigmoid2).astype(bf16)


def partner_of(me, offset, count):
    other = me
    bit = 1
    while bit < count:
        set_bit = (offset // bit) % 2
        other = other + set_bit * bit * (1 - 2 * ((me // bit) % 2))
        bit *= 2
    return other


def split_sources(n_ep):
    near = [d for d in range(1, n_ep) if d & (d - 1) == 0][::-1]
    far = [d for d in range(1, n_ep) if d & (d - 1) != 0][::-1]
    return near, far


def kernel(
    n_ep,
    n_tp,
    q_hbm,
    k_hbm,
    v_hbm,
    x_hbm,
    gain_hbm,
    ids_hbm,
    logits_hbm,
    gate_hbm,
    up_hbm,
    down_hbm,
    mixer_hbm,
    mix_out,
    routed_out,
    q_ref,
    k_ref,
    v_ref,
    x_ref,
    gain_ref,
    ids_ref,
    logits_ref,
    wg,
    wu,
    wd,
    wm,
    xs,
    xr,
    wr,
    kvr,
    pb,
    cr,
    sb,
    rr,
    zb,
    zr,
    at_send,
    at_recv,
    qt_ref,
    kv_ref,
    wt_ref,
    wc,
    acc,
    tot,
    hs,
    ob,
    ex,
    w_sem,
    in_sem,
    xf_ss,
    xf_rs,
    g_ss,
    g_rs,
    ff_ss,
    ff_rs,
    y_ss,
    y_rs,
    e_ss,
    e_rs,
    d_ss,
    cf_rs,
    d_rs,
    xn_ss,
    fn_ss,
    xn_rs,
    fn_rs,
    cn_rs,
    rn_rs,
    wt_rs,
    kv_ss,
    kv_rs,
    z_rs,
    a_rs,
    c0_rs,
    r_ss,
    c_ss,
    z_ss,
    a_ss,
    wt_ss,
):
    e = lax.axis_index("ep")
    t = lax.axis_index("tp")
    core = t % 2
    zi = t // 2
    zs = n_tp // 2
    mate = t + 1 - 2 * core
    heads, seqs, seg, hd = qt_ref.shape
    tokens, width = x_ref.shape
    half = tokens // 2
    quarter = tokens // 4
    zp = zi % 2
    zmate = t + 2 - 4 * zp
    slots = wt_ref.shape[1]
    local_experts = wg.shape[0]
    ch = width // n_tp
    pp = seg // n_tp
    near, distances = split_sources(n_ep)
    passes = len(near)
    count = len(distances)
    part = tokens // passes
    upper, lower = pl.ds(0, half), pl.ds(half, half)
    everything = slice(None)

    weights = [
        pltpu.make_async_copy(src, dst, w_sem.at[i])
        for i, (src, dst) in enumerate(
            ((gate_hbm, wg), (up_hbm, wu), (down_hbm, wd), (mixer_hbm, wm))
        )
    ]
    inputs = [
        pltpu.make_async_copy(src, dst, in_sem.at[i])
        for i, (src, dst) in enumerate(
            (
                (x_hbm, x_ref),
                (q_hbm, q_ref),
                (k_hbm, k_ref),
                (v_hbm, v_ref),
                (ids_hbm, ids_ref),
                (logits_hbm, logits_ref),
                (gain_hbm, gain_ref),
            )
        )
    ]

    def ep_peer(d):
        return partner_of(e, d, n_ep)

    barrier = pltpu.get_barrier_semaphore()
    for d in range(1, n_ep):
        pl.semaphore_signal(barrier, inc=1, device_id={"ep": ep_peer(d)}, device_id_type=MESH)
    for d in range(1, n_tp):
        pl.semaphore_signal(
            barrier, inc=1, device_id={"tp": (t + d) % n_tp}, device_id_type=MESH
        )
    for copy in inputs:
        copy.start()

    orders = [
        sorted((c for c in range(zs) if c != z), key=lambda c: -abs(c - z)) + [z]
        for z in range(zs)
    ]

    def chunk(k):
        return sum(jnp.where(zi == z, order[k - 1], 0) for z, order in enumerate(orders))

    def nth(i):
        return sum(jnp.where(i == n, d, 0) for n, d in enumerate(distances))

    def remote(src, dst, send, recv, axis, to):
        return pltpu.make_async_remote_copy(
            src_ref=src,
            dst_ref=dst,
            send_sem=send,
            recv_sem=recv,
            device_id={axis: to},
            device_id_type=MESH,
        )

    def settle_bytes(ref, sem):
        pltpu.make_async_copy(ref, ref, sem).wait()

    mine = pl.ds(pl.multiple_of(core * half, half), half)
    piece = pl.ds(pl.multiple_of(core * half + zp * quarter, quarter), quarter)

    def span(h):
        return pl.ds(pl.multiple_of(h * part, part), part)

    def own_part(h):
        return pl.ds(pl.multiple_of(h * part + core * (part // 2), part // 2), part // 2)

    def xf_copy(i):
        d = nth(i)
        return remote(xs.at[piece], xr.at[d, piece], xf_ss.at[i], xf_rs.at[i], "ep", ep_peer(d))

    def g_copy(i):
        ref = xr.at[nth(i), piece]
        return remote(ref, ref, g_ss.at[i], g_rs.at[i], "tp", zmate)

    def ff_copy(i):
        ref = xr.at[nth(i), mine]
        return remote(ref, ref, ff_ss.at[i], ff_rs.at[i], "tp", mate)

    def xn_copy(n, h):
        rows = own_part(h)
        return remote(
            xs.at[rows],
            xr.at[near[n], rows],
            xn_ss.at[n],
            xn_rs.at[n, h],
            "ep",
            ep_peer(near[n]),
        )

    def fn_copy(n, h):
        ref = xr.at[near[n], own_part(h)]
        return remote(ref, ref, fn_ss.at[n], fn_rs.at[n, h], "tp", mate)

    def wt_copy(d):
        return remote(
            wt_ref.at[ep_peer(d)], wr.at[d], wt_ss.at[0], wt_rs.at[d - 1], "ep", ep_peer(d)
        )

    def kv_copy(d):
        return remote(
            kv_ref, kvr.at[d], kv_ss.at[d - 1], kv_rs.at[d - 1], "ep", (e + d) % n_ep
        )

    def c_copy(d, c, rows, sem):
        return remote(
            pb.at[d, 1 - core, c, rows], cr.at[d, c, rows], c_ss.at[0], sem, "tp", mate
        )

    def r_copy(n, h, k):
        c = chunk(k)
        return remote(
            sb.at[near[n], c, span(h)],
            rr.at[near[n], c, span(h)],
            r_ss.at[0],
            rn_rs.at[n, h, k - 1],
            "ep",
            ep_peer(near[n]),
        )

    def y_copy(i, k):
        d = nth(i)
        c = chunk(k)
        return remote(
            sb.at[d, c, upper],
            rr.at[d, zi, upper],
            y_ss.at[i],
            y_rs.at[i],
            "tp",
            c * 2 + core,
        )

    def e_copy(i):
        d = nth(i)
        return remote(
            sb.at[d, zi, upper], ex.at[i], e_ss.at[i], e_rs.at[i], "ep", ep_peer(d)
        )

    def d_copy(i, k):
        d = nth(i)
        c = chunk(k)
        return remote(
            sb.at[d, c, lower],
            rr.at[d, c, lower],
            d_ss.at[i],
            d_rs.at[i, k - 1],
            "ep",
            ep_peer(d),
        )

    def z_copy(k, h):
        dz = chunk(k)
        return remote(
            zb.at[dz, span(h)],
            zr.at[zi, span(h)],
            z_ss.at[0],
            z_rs.at[0],
            "tp",
            dz * 2 + core,
        )

    def a_copy(d):
        to = (t + d) % n_tp
        return remote(at_send.at[to], at_recv.at[t], a_ss.at[0], a_rs.at[0], "tp", to)

    with scope("xload"):
        for copy in inputs:
            copy.wait()
    for copy in weights:
        copy.start()

    with scope("norm0"):
        values = x_ref[...].astype(f32)
        mean = jnp.mean(values * values, axis=-1, keepdims=True)
        xs[...] = (values * lax.rsqrt(mean + norm_eps) * gain_ref[...]).astype(bf16)

    top = ids_ref.shape[0]
    logits = [logits_ref[k : k + 1] for k in range(top)]
    peak = functools.reduce(jnp.maximum, logits)
    powers = [jnp.exp(value - peak) for value in logits]
    share = 1.0 / functools.reduce(jnp.add, powers)
    slot = lax.broadcasted_iota(jnp.int32, (slots, tokens), 0)
    for g in range(n_ep):
        expert = jnp.where(slot < local_experts, g * local_experts + slot, -1)
        table = jnp.zeros((slots, tokens), f32)
        for k in range(top):
            table = table + jnp.where(ids_ref[k : k + 1] == expert, powers[k] * share, 0.0)
        wt_ref[g] = table

    with scope("barrier"):
        pl.semaphore_wait(barrier, n_ep - 1 + n_tp - 1)
    for d in range(1, n_ep):
        wt_copy(d).start()
    for i in range(count):
        xf_copy(i).start()
    for n in range(passes):
        xn_copy(n, 0).start()

    rows = hd * seqs
    for s in range(seqs):
        pick = (
            (
                lax.broadcasted_iota(jnp.int32, (hd, rows), 1)
                == lax.broadcasted_iota(jnp.int32, (hd, rows), 0) * seqs + s
            )
            .astype(f32)
            .astype(bf16)
        )
        for h in range(heads):
            kv_ref[0, h, s] = jnp.dot(pick, k_ref[h], preferred_element_type=f32).astype(bf16)
            kv_ref[1, h, s] = jnp.dot(pick, v_ref[h], preferred_element_type=f32).astype(bf16)
            query = jnp.dot(pick, q_ref[h], preferred_element_type=f32)
            qt_ref[h, s] = query.T.astype(bf16)

    def up(j, lhs, columns):
        gate_pre = jnp.dot(lhs(), wg[j], preferred_element_type=f32)
        up_pre = jnp.dot(lhs(), wu[j], preferred_element_type=f32)
        hs[j] = activate(gate_pre, up_pre, columns[:, j : j + 1])

    def down(sources, rows, sem):
        size = tokens // len(sources)
        for k in range(1, zs + 1):
            c = chunk(k)
            for p in range(2):
                place = pl.ds(pl.multiple_of((2 * c + p) * ch, ch), ch)
                total = functools.reduce(
                    jnp.add,
                    [
                        jnp.dot(hs[j], wd[j, :, place], preferred_element_type=f32)
                        for j in range(local_experts)
                    ],
                ).astype(bf16)
                for n, d in enumerate(sources):
                    pb[d, p, c, rows] = total[n * size : (n + 1) * size]
        for k in range(1, zs + 1):
            for d in sources:
                c_copy(d, chunk(k), rows, sem).start()

    def joined(d, c, rows):
        sb[d, c, rows] = (pb[d, core, c, rows].astype(f32) + cr[d, c, rows].astype(f32)).astype(
            bf16
        )

    def finish_own():
        settle_bytes(cr.at[0], c0_rs.at[0])
        for c in range(zs):
            joined(0, c, everything)

    def finish_far(i):
        d = nth(i)
        settle_bytes(cr.at[d], cf_rs.at[i])
        for k in range(1, zs + 1):
            joined(d, chunk(k), everything)
            d_copy(i, k).start()
            if k < zs:
                y_copy(i, k).start()

    def finish_near(h):
        settle_bytes(cr.at[pl.ds(0, passes), :, span(h)], cn_rs.at[h])
        for k in range(1, zs + 1):
            for n in range(passes):
                joined(near[n], chunk(k), span(h))
                r_copy(n, h, k).start()

    def gathered(i):
        d = nth(i)
        settle_bytes(rr.at[d, pl.ds(0, zs - 1), upper], y_rs.at[i])
        total = sb[d, zi, upper].astype(f32)
        for k in range(1, zs):
            total = total + rr[d, chunk(k), upper].astype(f32)
        sb[d, zi, upper] = total.astype(bf16)
        e_copy(i).start()

    def settle(h):
        for k in range(1, zs + 1):
            c = chunk(k)
            own = sb[0, c, span(h)].astype(f32)
            for n in range(passes):
                r_copy(n, h, k).wait_recv()
                own = own + rr[near[n], c, span(h)].astype(f32)
            if h * part >= half:
                for i, d in enumerate(distances):
                    if h * part == half:
                        d_copy(i, k).wait_recv()
                    own = own + rr[d, c, span(h)].astype(f32)
            if k < zs:
                zb[c, span(h)] = own.astype(bf16)
                z_copy(k, h).start()
            else:
                ob[span(h)] = own

    pairs = heads * seqs
    tall = pairs * seg
    row_id = lax.broadcasted_iota(jnp.int32, (2 * seg, 2 * seg), 0) % seg
    col_id = lax.broadcasted_iota(jnp.int32, (2 * seg, 2 * seg), 1)
    later_mask = ((row_id > col_id) | (col_id >= seg)).astype(f32).astype(bf16)
    scale = hd ** (-0.5)

    def block(kv, diagonal):
        scores = jnp.concatenate(
            [
                jnp.dot(qt_ref[p // seqs, p % seqs], kv[0, p // seqs, p % seqs],
                        preferred_element_type=f32)
                for p in range(pairs)
            ],
            axis=0,
        ) * scale
        log_term = jnp.log(1.0 + jnp.exp(-jnp.abs(scores)))
        keep = -(jnp.maximum(scores, 0.0) + log_term)
        beta = jnp.minimum(scores, 0.0) - log_term
        if diagonal:
            usable = lax.broadcasted_iota(jnp.int32, (tall, seg), 1) < (
                lax.broadcasted_iota(jnp.int32, (tall, seg), 0) % seg
            )
            keep = jnp.where(usable, keep, 0.0)
        high = keep.astype(bf16)
        low = (keep - high.astype(f32)).astype(bf16)
        sums = jnp.dot(
            jnp.concatenate([high, low], axis=1), later_mask, preferred_element_type=f32
        )
        weight = jnp.exp(beta + sums[:, :seg])
        if diagonal:
            weight = jnp.where(usable, weight, 0.0)
        weight = weight.astype(bf16)
        out = jnp.concatenate(
            [
                lax.dot_general(
                    weight[p * seg : (p + 1) * seg],
                    kv[1, p // seqs, p % seqs],
                    (((1,), (1,)), ((), ())),
                    preferred_element_type=f32,
                )
                for p in range(pairs)
            ],
            axis=0,
        )
        return out, sums[:, seg : seg + hd]

    with scope("diag"):
        acc[...], tot[...] = block(kv_ref, True)

    def share_near(h):
        with scope("xwait"):
            for n in range(passes):
                xn_copy(n, h).wait_recv()
                fn_copy(n, h).start()

    def share_far(i):
        with scope("gwait"):
            g_copy(i).wait_recv()
            ff_copy(i).start()

    with scope("weights"):
        for copy in weights[:3]:
            copy.wait()
    own_columns = wt_ref[e].T
    with scope("up0"):
        up(0, lambda: xs[...], own_columns)
    with scope("waitfar"):
        for i in range(count):
            xf_copy(i).wait_recv()
            g_copy(i).start()
        for h in range(1, passes):
            for n in range(passes):
                xn_copy(n, h).start()
    with scope("up0"):
        for j in range(1, local_experts):
            up(j, lambda: xs[...], own_columns)
    share_near(0)
    with scope("down0"):
        down([0], everything, c0_rs.at[0])
    for k in range(1, n_ep):

        @pl.when(e + k < n_ep)
        def _():
            kv_copy(k).start()

    def near_pass(h, middle):
        with scope("fwait"):
            for n in range(passes):
                fn_copy(n, h).wait_recv()

        def lhs():
            return jnp.concatenate([xr[d, span(h)] for d in near], axis=0)

        columns = jnp.concatenate([wc[n, span(h)] for n in range(passes)], axis=0)
        for j in range(local_experts):
            with scope("up"):
                up(j, lhs, columns)
            if j == 0:
                middle()
        with scope("down"):
            down(near, span(h), cn_rs.at[h])

    def far_pass(i, middle):
        d = nth(i)
        with scope("fwait"):
            ff_copy(i).wait_recv()
            wt_copy(d).wait_recv()
        columns = wr[d].T
        for j in range(local_experts):
            with scope("up"):
                up(j, lambda: xr[d], columns)
            if j == 0:
                middle()
        with scope("downfar"):
            down([d], everything, cf_rs.at[i])

    def first_passes(h, carry):
        @pl.when(h > 0)
        def _():
            share_near(h)

        def middle():
            with scope("finish"):

                @pl.when(h > 0)
                def _():
                    finish_near(h - 1)

                @pl.when(h == 0)
                def _():
                    finish_own()

            if distances:

                @pl.when(h == passes - 2)
                def _():
                    share_far(0)

        near_pass(h, middle)
        return carry

    def far_passes(i, carry):
        def middle():
            @pl.when(i == 0)
            def _():
                with scope("finish"):
                    finish_near(passes - 2)

            @pl.when(i > 0)
            def _():
                finish_far(i - 1)

            @pl.when(i < count - 1)
            def _():
                share_far(i + 1)

            @pl.when(i == count - 1)
            def _():
                share_near(passes - 1)

        far_pass(i, middle)
        return carry

    def last_middle():
        with scope("finishfar"):
            if distances:
                finish_far(count - 1)
            else:
                finish_own()

    for n in range(passes):
        wt_copy(near[n]).wait_recv()
        wc[n] = wr[near[n]].T
    lax.fori_loop(0, passes - 1, first_passes, 0)
    lax.fori_loop(0, count, far_passes, 0)
    if not distances:
        share_near(passes - 1)
    near_pass(passes - 1, last_middle)
    with scope("finlast"):
        finish_near(passes - 1)

    def further(d, carry):
        kv_copy(d).wait_recv()
        out, total = block(kvr.at[d], False)
        later = tot[...]
        acc[...] = acc[...] + jnp.exp(later) * out
        tot[...] = later + total
        return carry

    with scope("further"):
        lax.fori_loop(1, e + 1, further, 0)
    with scope("asend"):
        for p in range(pairs):
            h, s = p // seqs, p % seqs
            for c in range(n_tp):
                at_send[c, s * pp : (s + 1) * pp, h * hd : (h + 1) * hd] = acc[
                    p * seg + c * pp : p * seg + (c + 1) * pp
                ].astype(bf16)
        for d in range(1, n_tp):
            a_copy(d).start()
        at_recv[t] = at_send[t]

    for h in range(passes):
        if h == passes - 1:
            with scope("gathered"):
                lax.fori_loop(0, count, lambda i, carry: (gathered(i), carry)[1], 0)
        with scope("settle"):
            settle(h)

    with scope("wmix"):
        weights[3].wait()
    with scope("await"):
        settle_bytes(at_recv.at[pl.ds(0, n_tp - 1)], a_rs.at[0])
    with scope("mix"):
        wide = jnp.concatenate([at_recv[c] for c in range(n_tp)], axis=1)
        mixed = jnp.dot(wide, wm[...], preferred_element_type=f32)
        for s in range(seqs):
            mix_out[s] = mixed[s * pp : (s + 1) * pp].astype(bf16)

    with scope("zfin"):
        settle_bytes(zr.at[pl.ds(0, zs - 1)], z_rs.at[0])
        for i, d in enumerate(distances):
            e_copy(i).wait_recv()
            ob[upper] = ob[upper] + ex[i].astype(f32)
        total = ob[...]
        for k in range(1, zs):
            total = total + zr[chunk(k)].astype(f32)
        routed_out[...] = total.T.astype(bf16)

    with scope("drain"):
        settle_bytes(wt_ref.at[pl.ds(0, n_ep - 1)], wt_ss.at[0])
        for i in range(count):
            xf_copy(i).wait_send()
            g_copy(i).wait_send()
            ff_copy(i).wait_send()
            settle_bytes(sb.at[0, pl.ds(0, zs - 1), upper], y_ss.at[i])
            settle_bytes(sb.at[0, :, upper], d_ss.at[i])
            e_copy(i).wait_send()
        for n in range(passes):
            settle_bytes(xs.at[mine], xn_ss.at[n])
            settle_bytes(xs.at[mine], fn_ss.at[n])
        settle_bytes(cr, c_ss.at[0])
        settle_bytes(sb.at[pl.ds(0, passes)], r_ss.at[0])
        settle_bytes(zb.at[pl.ds(0, zs - 1)], z_ss.at[0])
        settle_bytes(at_send.at[pl.ds(0, n_tp - 1)], a_ss.at[0])
        for k in range(1, n_ep):

            @pl.when(e + k < n_ep)
            def _():
                kv_copy(k).wait_send()


def hand_over(mixed_ref, routed_ref, mix_out, routed_out, sems):
    copies = [
        pltpu.make_async_copy(src, dst, sems.at[i])
        for i, (src, dst) in enumerate(((mixed_ref, mix_out), (routed_ref, routed_out)))
    ]
    for copy in copies:
        copy.start()
    for copy in copies:
        copy.wait()


def body(
    queries,
    key_vectors,
    value_vectors,
    mixer_weight,
    expert_rows,
    norm_gain,
    route_ids,
    route_logits,
    gate_weight,
    up_weight,
    down_weight,
):
    n_ep, n_tp = lax.axis_size("ep"), lax.axis_size("tp")
    heads, hd, seqs, seg = queries.shape
    tokens, width = expert_rows.shape
    local_experts, _, ff = gate_weight.shape
    zs, ch, pp = n_tp // 2, width // n_tp, seg // n_tp

    top = route_ids.shape[1]
    slots = 8 * -(-local_experts // 8)
    pairs = heads * seqs
    near, distances = split_sources(n_ep)
    passes, count = len(near), max(len(distances), 1)
    kv_shape = (2, heads, seqs, hd, seg)

    def merged(rows):
        return rows.reshape(heads, hd * seqs, seg)

    vmem = pl.BlockSpec(memory_space=pltpu.VMEM)
    anywhere = pl.BlockSpec(memory_space=pltpu.HBM)
    dma = pltpu.SemaphoreType.DMA
    outs = 2 * seqs * pp * width + 2 * ch * tokens
    limit = (60 * 1024 * 1024) - outs - (64 << 10)
    shapes = ((seqs, pp, width), (ch, tokens))
    results = pl.pallas_call(
        functools.partial(kernel, n_ep, n_tp),
        out_shape=tuple(pltpu.VMEM(shape, bf16) for shape in shapes),
        in_specs=[anywhere] * 11,
        out_specs=(vmem, vmem),
        scratch_shapes=[
            pltpu.VMEM((heads, hd * seqs, seg), bf16),
            pltpu.VMEM((heads, hd * seqs, seg), bf16),
            pltpu.VMEM((heads, hd * seqs, seg), bf16),
            pltpu.VMEM((tokens, width), bf16),
            pltpu.VMEM((1, width), f32),
            pltpu.VMEM((top, tokens), jnp.int32),
            pltpu.VMEM((top, tokens), f32),
            pltpu.VMEM(gate_weight.shape, bf16),
            pltpu.VMEM(up_weight.shape, bf16),
            pltpu.VMEM(down_weight.shape, bf16),
            pltpu.VMEM(mixer_weight.shape, bf16),
            pltpu.VMEM((tokens, width), bf16),
            pltpu.VMEM((n_ep, tokens, width), bf16),
            pltpu.VMEM((n_ep, slots, tokens), f32),
            pltpu.VMEM((n_ep,) + kv_shape, bf16),
            pltpu.VMEM((n_ep, 2, zs, tokens, ch), bf16),
            pltpu.VMEM((n_ep, zs, tokens, ch), bf16),
            pltpu.VMEM((n_ep, zs, tokens, ch), bf16),
            pltpu.VMEM((n_ep, zs, tokens, ch), bf16),
            pltpu.VMEM((zs, tokens, ch), bf16),
            pltpu.VMEM((zs, tokens, ch), bf16),
            pltpu.VMEM((n_tp, seqs * pp, heads * hd), bf16),
            pltpu.VMEM((n_tp, seqs * pp, heads * hd), bf16),
            pltpu.VMEM((heads, seqs, seg, hd), bf16),
            pltpu.VMEM(kv_shape, bf16),
            pltpu.VMEM((n_ep, slots, tokens), f32),
            pltpu.VMEM((passes, tokens, slots), f32),
            pltpu.VMEM((pairs * seg, hd), f32),
            pltpu.VMEM((pairs * seg, hd), f32),
            pltpu.VMEM((local_experts, tokens, ff), bf16),
            pltpu.VMEM((tokens, ch), f32),
            pltpu.VMEM((count, tokens // 2, ch), bf16),
            dma((4,)),
            dma((7,)),
        ]
        + [dma((count,))] * 12
        + [dma((count, zs))]
        + [dma((passes,))] * 2
        + [dma((passes, passes))] * 2
        + [dma((passes,)), dma((passes, passes, zs))]
        + [dma((n_ep - 1,))] * 3
        + [dma((1,))] * 8,
        compiler_params=pltpu.CompilerParams(
            collective_id=0, has_side_effects=True, vmem_limit_bytes=limit
        ),
    )(
        merged(queries),
        merged(key_vectors),
        merged(value_vectors),
        expert_rows,
        norm_gain[None, :],
        route_ids.T,
        route_logits.T,
        gate_weight,
        up_weight,
        down_weight,
        mixer_weight,
    )
    return pl.pallas_call(
        hand_over,
        out_shape=tuple(jax.ShapeDtypeStruct(shape, bf16) for shape in shapes),
        in_specs=[vmem] * 2,
        out_specs=(anywhere, anywhere),
        scratch_shapes=[dma((2,))],
        compiler_params=pltpu.CompilerParams(vmem_limit_bytes=1 << 20),
    )(*results)


def solution(mesh):
    in_specs = (
        P("tp", None, None, "ep"),
        P("tp", None, None, "ep"),
        P("tp", None, None, "ep"),
        P(),
        P("ep", None),
        P(),
        P("ep", None),
        P("ep", None),
        P("ep", None, "tp"),
        P("ep", None, "tp"),
        P("ep", "tp", None),
    )
    out_specs = (P(None, ("ep", "tp"), None), P("tp", "ep"))
    return jax.shard_map(body, mesh=mesh, in_specs=in_specs, out_specs=out_specs, check_vma=False)
```

```python
import functools

import jax
import jax.numpy as jnp
from jax import lax
from jax.experimental import pallas as pl
from jax.experimental.pallas import tpu as pltpu
from jax.sharding import PartitionSpec as P

limit_value = 7.0
alpha_value = 1.702
norm_eps = 1e-06

MESH = pl.DeviceIdType.MESH
f32 = jnp.float32
bf16 = jnp.bfloat16
scope = jax.named_scope


def activate(gate_pre, up_pre, weight):
    g = jnp.minimum(gate_pre, limit_value)
    u = jnp.clip(up_pre, -limit_value, limit_value)
    sigmoid2 = 1.0 + jnp.tanh((0.5 * alpha_value) * g)
    return ((u + 1.0) * (g * (0.5 * weight)) * sigmoid2).astype(bf16)


def partner_of(me, offset, count):
    other = me
    bit = 1
    while bit < count:
        set_bit = (offset // bit) % 2
        other = other + set_bit * bit * (1 - 2 * ((me // bit) % 2))
        bit *= 2
    return other


def split_sources(n_ep):
    near = [d for d in range(1, n_ep) if d & (d - 1) == 0][::-1]
    far = [d for d in range(1, n_ep) if d & (d - 1) != 0][::-1]
    return near, far


def kernel(
    n_ep,
    n_tp,
    q_hbm,
    k_hbm,
    v_hbm,
    x_hbm,
    gain_hbm,
    ids_hbm,
    logits_hbm,
    gate_hbm,
    up_hbm,
    down_hbm,
    mixer_hbm,
    mix_out,
    routed_out,
    q_ref,
    k_ref,
    v_ref,
    x_ref,
    gain_ref,
    ids_ref,
    logits_ref,
    wg,
    wu,
    wd,
    wm,
    xs,
    xr,
    wr,
    kvr,
    pb,
    cr,
    sb,
    rr,
    zb,
    zr,
    at_send,
    at_recv,
    qt_ref,
    kv_ref,
    wt_ref,
    wc,
    acc,
    tot,
    hs,
    ob,
    ex,
    w_sem,
    in_sem,
    xf_ss,
    xf_rs,
    g_ss,
    g_rs,
    ff_ss,
    ff_rs,
    y_ss,
    y_rs,
    e_ss,
    e_rs,
    d_ss,
    cf_rs,
    d_rs,
    xn_ss,
    fn_ss,
    xn_rs,
    fn_rs,
    cn_rs,
    rn_rs,
    wt_rs,
    kv_ss,
    kv_rs,
    z_rs,
    a_rs,
    c0_rs,
    r_ss,
    c_ss,
    z_ss,
    a_ss,
    wt_ss,
    wave,
):
    e = lax.axis_index("ep")
    t = lax.axis_index("tp")
    core = t % 2
    zi = t // 2
    zs = n_tp // 2
    mate = t + 1 - 2 * core
    heads, seqs, seg, hd = qt_ref.shape
    tokens, width = x_ref.shape
    half = tokens // 2
    quarter = tokens // 4
    zp = zi % 2
    zmate = t + 2 - 4 * zp
    slots = wt_ref.shape[1]
    local_experts = wg.shape[0]
    ch = width // n_tp
    pp = seg // n_tp
    near, distances = split_sources(n_ep)
    passes = len(near)
    count = len(distances)
    part = tokens // passes
    upper, lower = pl.ds(0, half), pl.ds(half, half)
    everything = slice(None)

    weights = [
        pltpu.make_async_copy(src, dst, w_sem.at[i])
        for i, (src, dst) in enumerate(
            ((gate_hbm, wg), (up_hbm, wu), (down_hbm, wd), (mixer_hbm, wm))
        )
    ]
    inputs = [
        pltpu.make_async_copy(src, dst, in_sem.at[i])
        for i, (src, dst) in enumerate(
            (
                (x_hbm, x_ref),
                (q_hbm, q_ref),
                (k_hbm, k_ref),
                (v_hbm, v_ref),
                (ids_hbm, ids_ref),
                (logits_hbm, logits_ref),
                (gain_hbm, gain_ref),
            )
        )
    ]

    def ep_peer(d):
        return partner_of(e, d, n_ep)

    barrier = pltpu.get_barrier_semaphore()
    for d in range(1, n_ep):
        pl.semaphore_signal(barrier, inc=1, device_id={"ep": ep_peer(d)}, device_id_type=MESH)
    below, above = zi > 0, zi < zs - 1
    greeted = n_ep + below.astype(jnp.int32) + above.astype(jnp.int32)

    def signal(sem, to):
        pl.semaphore_signal(sem, inc=1, device_id={"tp": to}, device_id_type=MESH)

    signal(barrier, mate)

    @pl.when(below)
    def _():
        signal(barrier, t - 2)

    @pl.when(above)
    def _():
        signal(barrier, t + 2)

    def wave_start():
        @pl.when(jnp.logical_not(above))
        def _():
            signal(wave.at[0], t - 2)

        @pl.when(jnp.logical_not(below))
        def _():
            signal(wave.at[1], t + 2)

    def wave_pass(way):
        @pl.when(below & above)
        def _():
            pl.semaphore_wait(wave.at[way], 1)
            signal(wave.at[way], t + 4 * way - 2)

    def wave_end():
        @pl.when(jnp.logical_not(below))
        def _():
            pl.semaphore_wait(wave.at[0], 1)

        @pl.when(jnp.logical_not(above))
        def _():
            pl.semaphore_wait(wave.at[1], 1)

    for copy in inputs:
        copy.start()

    orders = [
        sorted((c for c in range(zs) if c != z), key=lambda c: -abs(c - z)) + [z]
        for z in range(zs)
    ]

    def chunk(k):
        return sum(jnp.where(zi == z, order[k - 1], 0) for z, order in enumerate(orders))

    def nth(i):
        return sum(jnp.where(i == n, d, 0) for n, d in enumerate(distances))

    def remote(src, dst, send, recv, axis, to):
        return pltpu.make_async_remote_copy(
            src_ref=src,
            dst_ref=dst,
            send_sem=send,
            recv_sem=recv,
            device_id={axis: to},
            device_id_type=MESH,
        )

    def settle_bytes(ref, sem):
        pltpu.make_async_copy(ref, ref, sem).wait()

    mine = pl.ds(pl.multiple_of(core * half, half), half)
    piece = pl.ds(pl.multiple_of(core * half + zp * quarter, quarter), quarter)

    def span(h):
        return pl.ds(pl.multiple_of(h * part, part), part)

    def own_part(h):
        return pl.ds(pl.multiple_of(h * part + core * (part // 2), part // 2), part // 2)

    def xf_copy(i):
        d = nth(i)
        return remote(xs.at[piece], xr.at[d, piece], xf_ss.at[i], xf_rs.at[i], "ep", ep_peer(d))

    def g_copy(i):
        ref = xr.at[nth(i), piece]
        return remote(ref, ref, g_ss.at[i], g_rs.at[i], "tp", zmate)

    def ff_copy(i):
        ref = xr.at[nth(i), mine]
        return remote(ref, ref, ff_ss.at[i], ff_rs.at[i], "tp", mate)

    def xn_copy(n, h):
        rows = own_part(h)
        return remote(
            xs.at[rows],
            xr.at[near[n], rows],
            xn_ss.at[n],
            xn_rs.at[n, h],
            "ep",
            ep_peer(near[n]),
        )

    def fn_copy(n, h):
        ref = xr.at[near[n], own_part(h)]
        return remote(ref, ref, fn_ss.at[n], fn_rs.at[n, h], "tp", mate)

    def wt_copy(d):
        return remote(
            wt_ref.at[ep_peer(d)], wr.at[d], wt_ss.at[0], wt_rs.at[d - 1], "ep", ep_peer(d)
        )

    def kv_copy(d):
        return remote(
            kv_ref, kvr.at[d], kv_ss.at[d - 1], kv_rs.at[d - 1], "ep", (e + d) % n_ep
        )

    def c_copy(d, c, rows, sem):
        return remote(
            pb.at[d, 1 - core, c, rows], cr.at[d, c, rows], c_ss.at[0], sem, "tp", mate
        )

    def r_copy(n, h, k):
        c = chunk(k)
        return remote(
            sb.at[near[n], c, span(h)],
            rr.at[near[n], c, span(h)],
            r_ss.at[0],
            rn_rs.at[h, k - 1],
            "ep",
            ep_peer(near[n]),
        )

    def y_copy(i, k):
        d = nth(i)
        c = chunk(k)
        return remote(
            sb.at[d, c, upper],
            rr.at[d, zi, upper],
            y_ss.at[i],
            y_rs.at[i],
            "tp",
            c * 2 + core,
        )

    def e_copy(i):
        d = nth(i)
        return remote(
            sb.at[d, zi, upper], ex.at[i], e_ss.at[i], e_rs.at[i], "ep", ep_peer(d)
        )

    def d_copy(i, k):
        d = nth(i)
        c = chunk(k)
        return remote(
            sb.at[d, c, lower],
            rr.at[d, c, lower],
            d_ss.at[i],
            d_rs.at[i, k - 1],
            "ep",
            ep_peer(d),
        )

    def z_copy(k, h):
        dz = chunk(k)
        return remote(
            zb.at[dz, span(h)],
            zr.at[zi, span(h)],
            z_ss.at[0],
            z_rs.at[0],
            "tp",
            dz * 2 + core,
        )

    def a_copy(d):
        to = (t + d) % n_tp
        return remote(at_send.at[to], at_recv.at[t], a_ss.at[0], a_rs.at[0], "tp", to)

    with scope("xload"):
        for copy in inputs:
            copy.wait()
    for copy in weights:
        copy.start()

    with scope("norm0"):
        values = x_ref[...].astype(f32)
        mean = jnp.mean(values * values, axis=-1, keepdims=True)
        xs[...] = (values * lax.rsqrt(mean + norm_eps) * gain_ref[...]).astype(bf16)

    top = ids_ref.shape[0]
    logits = [logits_ref[k : k + 1] for k in range(top)]
    peak = functools.reduce(jnp.maximum, logits)
    powers = [jnp.exp(value - peak) for value in logits]
    share = 1.0 / functools.reduce(jnp.add, powers)
    slot = lax.broadcasted_iota(jnp.int32, (slots, tokens), 0)
    for g in range(n_ep):
        expert = jnp.where(slot < local_experts, g * local_experts + slot, -1)
        table = jnp.zeros((slots, tokens), f32)
        for k in range(top):
            table = table + jnp.where(ids_ref[k : k + 1] == expert, powers[k] * share, 0.0)
        wt_ref[g] = table

    with scope("barrier"):
        pl.semaphore_wait(barrier, greeted)
    for d in range(1, n_ep):
        wt_copy(d).start()
    for i in range(count):
        xf_copy(i).start()
    for n in range(passes):
        xn_copy(n, 0).start()
    wave_start()

    rows = hd * seqs
    for s in range(seqs):
        pick = (
            (
                lax.broadcasted_iota(jnp.int32, (hd, rows), 1)
                == lax.broadcasted_iota(jnp.int32, (hd, rows), 0) * seqs + s
            )
            .astype(f32)
            .astype(bf16)
        )
        for h in range(heads):
            kv_ref[0, h, s] = jnp.dot(pick, k_ref[h], preferred_element_type=f32).astype(bf16)
            kv_ref[1, h, s] = jnp.dot(pick, v_ref[h], preferred_element_type=f32).astype(bf16)
            query = jnp.dot(pick, q_ref[h], preferred_element_type=f32)
            qt_ref[h, s] = query.T.astype(bf16)

    def up(j, lhs, columns):
        gate_pre = jnp.dot(lhs(), wg[j], preferred_element_type=f32)
        up_pre = jnp.dot(lhs(), wu[j], preferred_element_type=f32)
        hs[j] = activate(gate_pre, up_pre, columns[:, j : j + 1])

    def down(sources, rows, sem):
        size = tokens // len(sources)
        for k in range(1, zs + 1):
            c = chunk(k)
            for p in range(2):
                place = pl.ds(pl.multiple_of((2 * c + p) * ch, ch), ch)
                total = functools.reduce(
                    jnp.add,
                    [
                        jnp.dot(hs[j], wd[j, :, place], preferred_element_type=f32)
                        for j in range(local_experts)
                    ],
                ).astype(bf16)
                for n, d in enumerate(sources):
                    pb[d, p, c, rows] = total[n * size : (n + 1) * size]
        for k in range(1, zs + 1):
            for d in sources:
                c_copy(d, chunk(k), rows, sem).start()

    def joined(d, c, rows):
        sb[d, c, rows] = (pb[d, core, c, rows].astype(f32) + cr[d, c, rows].astype(f32)).astype(
            bf16
        )

    def finish_own():
        settle_bytes(cr.at[0], c0_rs.at[0])
        for c in range(zs):
            joined(0, c, everything)

    def finish_far(i):
        d = nth(i)
        settle_bytes(cr.at[d], cf_rs.at[i])
        for k in range(1, zs + 1):
            joined(d, chunk(k), everything)
            d_copy(i, k).start()
            if k < zs:
                y_copy(i, k).start()

    def finish_near(h):
        settle_bytes(cr.at[pl.ds(0, passes), :, span(h)], cn_rs.at[h])
        for k in range(1, zs + 1):
            for n in range(passes):
                joined(near[n], chunk(k), span(h))
                r_copy(n, h, k).start()

    def gathered(i):
        d = nth(i)
        settle_bytes(rr.at[d, pl.ds(0, zs - 1), upper], y_rs.at[i])
        total = sb[d, zi, upper].astype(f32)
        for k in range(1, zs):
            total = total + rr[d, chunk(k), upper].astype(f32)
        sb[d, zi, upper] = total.astype(bf16)
        e_copy(i).start()

    def settle(h):
        for k in range(1, zs + 1):
            c = chunk(k)
            own = sb[0, c, span(h)].astype(f32)
            settle_bytes(rr.at[pl.ds(0, passes), c, span(h)], rn_rs.at[h, k - 1])
            for n in range(passes):
                own = own + rr[near[n], c, span(h)].astype(f32)
            if h * part >= half:
                for i, d in enumerate(distances):
                    if h * part == half:
                        d_copy(i, k).wait_recv()
                    own = own + rr[d, c, span(h)].astype(f32)
            if k < zs:
                zb[c, span(h)] = own.astype(bf16)
                z_copy(k, h).start()
            else:
                ob[span(h)] = own

    pairs = heads * seqs
    tall = pairs * seg
    row_id = lax.broadcasted_iota(jnp.int32, (2 * seg, 2 * seg), 0) % seg
    col_id = lax.broadcasted_iota(jnp.int32, (2 * seg, 2 * seg), 1)
    later_mask = ((row_id > col_id) | (col_id >= seg)).astype(f32).astype(bf16)
    scale = hd ** (-0.5)

    def block(kv, diagonal):
        scores = jnp.concatenate(
            [
                jnp.dot(qt_ref[p // seqs, p % seqs], kv[0, p // seqs, p % seqs],
                        preferred_element_type=f32)
                for p in range(pairs)
            ],
            axis=0,
        ) * scale
        log_term = jnp.log(1.0 + jnp.exp(-jnp.abs(scores)))
        keep = -(jnp.maximum(scores, 0.0) + log_term)
        beta = jnp.minimum(scores, 0.0) - log_term
        if diagonal:
            usable = lax.broadcasted_iota(jnp.int32, (tall, seg), 1) < (
                lax.broadcasted_iota(jnp.int32, (tall, seg), 0) % seg
            )
            keep = jnp.where(usable, keep, 0.0)
        high = keep.astype(bf16)
        low = (keep - high.astype(f32)).astype(bf16)
        sums = jnp.dot(
            jnp.concatenate([high, low], axis=1), later_mask, preferred_element_type=f32
        )
        weight = jnp.exp(beta + sums[:, :seg])
        if diagonal:
            weight = jnp.where(usable, weight, 0.0)
        weight = weight.astype(bf16)
        out = jnp.concatenate(
            [
                lax.dot_general(
                    weight[p * seg : (p + 1) * seg],
                    kv[1, p // seqs, p % seqs],
                    (((1,), (1,)), ((), ())),
                    preferred_element_type=f32,
                )
                for p in range(pairs)
            ],
            axis=0,
        )
        return out, sums[:, seg : seg + hd]

    with scope("diag"):
        acc[...], tot[...] = block(kv_ref, True)

    def share_near(h):
        with scope("xwait"):
            for n in range(passes):
                xn_copy(n, h).wait_recv()
                fn_copy(n, h).start()

    def share_far(i):
        with scope("gwait"):
            g_copy(i).wait_recv()
            ff_copy(i).start()

    with scope("weights"):
        for copy in weights[:3]:
            copy.wait()
    own_columns = wt_ref[e].T
    with scope("up0"):
        up(0, lambda: xs[...], own_columns)
    with scope("waitfar"):
        for i in range(count):
            xf_copy(i).wait_recv()
            g_copy(i).start()
        for h in range(1, passes):
            for n in range(passes):
                xn_copy(n, h).start()
    with scope("up0"):
        for j in range(1, local_experts):
            up(j, lambda: xs[...], own_columns)
    share_near(0)
    with scope("down0"):
        down([0], everything, c0_rs.at[0])
    for k in range(1, n_ep):

        @pl.when(e + k < n_ep)
        def _():
            kv_copy(k).start()

    with scope("wave"):
        wave_pass(1)

    def near_pass(h, middle):
        with scope("fwait"):
            for n in range(passes):
                fn_copy(n, h).wait_recv()

        def lhs():
            return jnp.concatenate([xr[d, span(h)] for d in near], axis=0)

        columns = jnp.concatenate([wc[n, span(h)] for n in range(passes)], axis=0)
        for j in range(local_experts):
            with scope("up"):
                up(j, lhs, columns)
            if j == 0:
                middle()
        with scope("down"):
            down(near, span(h), cn_rs.at[h])

    def far_pass(i, middle):
        d = nth(i)
        with scope("fwait"):
            ff_copy(i).wait_recv()
            wt_copy(d).wait_recv()
        columns = wr[d].T
        for j in range(local_experts):
            with scope("up"):
                up(j, lambda: xr[d], columns)
            if j == 0:
                middle()
        with scope("downfar"):
            down([d], everything, cf_rs.at[i])

    def first_passes(h, carry):
        @pl.when(h > 0)
        def _():
            share_near(h)

        def middle():
            with scope("finish"):

                @pl.when(h > 0)
                def _():
                    finish_near(h - 1)

                @pl.when(h == 0)
                def _():
                    finish_own()

            if distances:

                @pl.when(h == passes - 2)
                def _():
                    share_far(0)

        near_pass(h, middle)
        return carry

    def far_passes(i, carry):
        def middle():
            @pl.when(i == 0)
            def _():
                with scope("finish"):
                    finish_near(passes - 2)

            @pl.when(i > 0)
            def _():
                finish_far(i - 1)

            @pl.when(i < count - 1)
            def _():
                share_far(i + 1)

            @pl.when(i == count - 1)
            def _():
                share_near(passes - 1)

        far_pass(i, middle)
        return carry

    def last_middle():
        with scope("finishfar"):
            if distances:
                finish_far(count - 1)
            else:
                finish_own()

    for n in range(passes):
        wt_copy(near[n]).wait_recv()
        wc[n] = wr[near[n]].T
    lax.fori_loop(0, passes - 1, first_passes, 0)
    with scope("wave"):
        wave_pass(0)
    lax.fori_loop(0, count, far_passes, 0)
    if not distances:
        share_near(passes - 1)
    with scope("wavend"):
        wave_end()
    near_pass(passes - 1, last_middle)
    with scope("finlast"):
        finish_near(passes - 1)

    def further(d, carry):
        kv_copy(d).wait_recv()
        out, total = block(kvr.at[d], False)
        later = tot[...]
        acc[...] = acc[...] + jnp.exp(later) * out
        tot[...] = later + total
        return carry

    with scope("further"):
        lax.fori_loop(1, e + 1, further, 0)
    with scope("asend"):
        for p in range(pairs):
            h, s = p // seqs, p % seqs
            for c in range(n_tp):
                at_send[c, s * pp : (s + 1) * pp, h * hd : (h + 1) * hd] = acc[
                    p * seg + c * pp : p * seg + (c + 1) * pp
                ].astype(bf16)
        for d in range(1, n_tp):
            a_copy(d).start()
        at_recv[t] = at_send[t]

    for h in range(passes):
        if h == passes - 1:
            with scope("gathered"):
                lax.fori_loop(0, count, lambda i, carry: (gathered(i), carry)[1], 0)
        with scope("settle"):
            settle(h)

    with scope("wmix"):
        weights[3].wait()
    with scope("await"):
        settle_bytes(at_recv.at[pl.ds(0, n_tp - 1)], a_rs.at[0])
    with scope("mix"):
        wide = jnp.concatenate([at_recv[c] for c in range(n_tp)], axis=1)
        mixed = jnp.dot(wide, wm[...], preferred_element_type=f32)
        for s in range(seqs):
            mix_out[s] = mixed[s * pp : (s + 1) * pp].astype(bf16)

    with scope("zfin"):
        settle_bytes(zr.at[pl.ds(0, zs - 1)], z_rs.at[0])
        for i, d in enumerate(distances):
            e_copy(i).wait_recv()
            ob[upper] = ob[upper] + ex[i].astype(f32)
        total = ob[...]
        for k in range(1, zs):
            total = total + zr[chunk(k)].astype(f32)
        routed_out[...] = total.T.astype(bf16)

    with scope("drain"):
        settle_bytes(wt_ref.at[pl.ds(0, n_ep - 1)], wt_ss.at[0])
        for i in range(count):
            xf_copy(i).wait_send()
            g_copy(i).wait_send()
            ff_copy(i).wait_send()
            settle_bytes(sb.at[0, pl.ds(0, zs - 1), upper], y_ss.at[i])
            settle_bytes(sb.at[0, :, upper], d_ss.at[i])
            e_copy(i).wait_send()
        for n in range(passes):
            settle_bytes(xs.at[mine], xn_ss.at[n])
            settle_bytes(xs.at[mine], fn_ss.at[n])
        settle_bytes(cr, c_ss.at[0])
        settle_bytes(sb.at[pl.ds(0, passes)], r_ss.at[0])
        settle_bytes(zb.at[pl.ds(0, zs - 1)], z_ss.at[0])
        settle_bytes(at_send.at[pl.ds(0, n_tp - 1)], a_ss.at[0])
        for k in range(1, n_ep):

            @pl.when(e + k < n_ep)
            def _():
                kv_copy(k).wait_send()


def hand_over(mixed_ref, routed_ref, mix_out, routed_out, sems):
    copies = [
        pltpu.make_async_copy(src, dst, sems.at[i])
        for i, (src, dst) in enumerate(((mixed_ref, mix_out), (routed_ref, routed_out)))
    ]
    for copy in copies:
        copy.start()
    for copy in copies:
        copy.wait()


def body(
    queries,
    key_vectors,
    value_vectors,
    mixer_weight,
    expert_rows,
    norm_gain,
    route_ids,
    route_logits,
    gate_weight,
    up_weight,
    down_weight,
):
    n_ep, n_tp = lax.axis_size("ep"), lax.axis_size("tp")
    heads, hd, seqs, seg = queries.shape
    tokens, width = expert_rows.shape
    local_experts, _, ff = gate_weight.shape
    zs, ch, pp = n_tp // 2, width // n_tp, seg // n_tp

    top = route_ids.shape[1]
    slots = 8 * -(-local_experts // 8)
    pairs = heads * seqs
    near, distances = split_sources(n_ep)
    passes, count = len(near), max(len(distances), 1)
    kv_shape = (2, heads, seqs, hd, seg)

    def merged(rows):
        return rows.reshape(heads, hd * seqs, seg)

    vmem = pl.BlockSpec(memory_space=pltpu.VMEM)
    anywhere = pl.BlockSpec(memory_space=pltpu.HBM)
    dma = pltpu.SemaphoreType.DMA
    outs = 2 * seqs * pp * width + 2 * ch * tokens
    limit = (60 * 1024 * 1024) - outs - (64 << 10)
    shapes = ((seqs, pp, width), (ch, tokens))
    results = pl.pallas_call(
        functools.partial(kernel, n_ep, n_tp),
        out_shape=tuple(pltpu.VMEM(shape, bf16) for shape in shapes),
        in_specs=[anywhere] * 11,
        out_specs=(vmem, vmem),
        scratch_shapes=[
            pltpu.VMEM((heads, hd * seqs, seg), bf16),
            pltpu.VMEM((heads, hd * seqs, seg), bf16),
            pltpu.VMEM((heads, hd * seqs, seg), bf16),
            pltpu.VMEM((tokens, width), bf16),
            pltpu.VMEM((1, width), f32),
            pltpu.VMEM((top, tokens), jnp.int32),
            pltpu.VMEM((top, tokens), f32),
            pltpu.VMEM(gate_weight.shape, bf16),
            pltpu.VMEM(up_weight.shape, bf16),
            pltpu.VMEM(down_weight.shape, bf16),
            pltpu.VMEM(mixer_weight.shape, bf16),
            pltpu.VMEM((tokens, width), bf16),
            pltpu.VMEM((n_ep, tokens, width), bf16),
            pltpu.VMEM((n_ep, slots, tokens), f32),
            pltpu.VMEM((n_ep,) + kv_shape, bf16),
            pltpu.VMEM((n_ep, 2, zs, tokens, ch), bf16),
            pltpu.VMEM((n_ep, zs, tokens, ch), bf16),
            pltpu.VMEM((n_ep, zs, tokens, ch), bf16),
            pltpu.VMEM((n_ep, zs, tokens, ch), bf16),
            pltpu.VMEM((zs, tokens, ch), bf16),
            pltpu.VMEM((zs, tokens, ch), bf16),
            pltpu.VMEM((n_tp, seqs * pp, heads * hd), bf16),
            pltpu.VMEM((n_tp, seqs * pp, heads * hd), bf16),
            pltpu.VMEM((heads, seqs, seg, hd), bf16),
            pltpu.VMEM(kv_shape, bf16),
            pltpu.VMEM((n_ep, slots, tokens), f32),
            pltpu.VMEM((passes, tokens, slots), f32),
            pltpu.VMEM((pairs * seg, hd), f32),
            pltpu.VMEM((pairs * seg, hd), f32),
            pltpu.VMEM((local_experts, tokens, ff), bf16),
            pltpu.VMEM((tokens, ch), f32),
            pltpu.VMEM((count, tokens // 2, ch), bf16),
            dma((4,)),
            dma((7,)),
        ]
        + [dma((count,))] * 12
        + [dma((count, zs))]
        + [dma((passes,))] * 2
        + [dma((passes, passes))] * 2
        + [dma((passes,)), dma((passes, zs))]
        + [dma((n_ep - 1,))] * 3
        + [dma((1,))] * 8
        + [pltpu.SemaphoreType.REGULAR((2,))],
        compiler_params=pltpu.CompilerParams(
            collective_id=0, has_side_effects=True, vmem_limit_bytes=limit
        ),
    )(
        merged(queries),
        merged(key_vectors),
        merged(value_vectors),
        expert_rows,
        norm_gain[None, :],
        route_ids.T,
        route_logits.T,
        gate_weight,
        up_weight,
        down_weight,
        mixer_weight,
    )
    return pl.pallas_call(
        hand_over,
        out_shape=tuple(jax.ShapeDtypeStruct(shape, bf16) for shape in shapes),
        in_specs=[vmem] * 2,
        out_specs=(anywhere, anywhere),
        scratch_shapes=[dma((2,))],
        compiler_params=pltpu.CompilerParams(vmem_limit_bytes=1 << 20),
    )(*results)


def solution(mesh):
    in_specs = (
        P("tp", None, None, "ep"),
        P("tp", None, None, "ep"),
        P("tp", None, None, "ep"),
        P(),
        P("ep", None),
        P(),
        P("ep", None),
        P("ep", None),
        P("ep", None, "tp"),
        P("ep", None, "tp"),
        P("ep", "tp", None),
    )
    out_specs = (P(None, ("ep", "tp"), None), P("tp", "ep"))
    return jax.shard_map(body, mesh=mesh, in_specs=in_specs, out_specs=out_specs, check_vma=False)
```

```python
import functools

import jax
import jax.numpy as jnp
from jax import lax
from jax.experimental import pallas as pl
from jax.experimental.pallas import tpu as pltpu
from jax.sharding import PartitionSpec as P

limit_value = 7.0
alpha_value = 1.702
norm_eps = 1e-06

MESH = pl.DeviceIdType.MESH
f32 = jnp.float32
bf16 = jnp.bfloat16
scope = jax.named_scope


def activate(gate_pre, up_pre, weight):
    g = jnp.minimum(gate_pre, limit_value)
    u = jnp.clip(up_pre, -limit_value, limit_value)
    sigmoid2 = 1.0 + jnp.tanh((0.5 * alpha_value) * g)
    return ((u + 1.0) * (g * (0.5 * weight)) * sigmoid2).astype(bf16)


def partner_of(me, offset, count):
    other = me
    bit = 1
    while bit < count:
        set_bit = (offset // bit) % 2
        other = other + set_bit * bit * (1 - 2 * ((me // bit) % 2))
        bit *= 2
    return other


def split_sources(n_ep):
    near = [d for d in range(1, n_ep) if d & (d - 1) == 0][::-1]
    far = [d for d in range(1, n_ep) if d & (d - 1) != 0][::-1]
    return near, far


def kernel(
    n_ep,
    n_tp,
    q_hbm,
    k_hbm,
    v_hbm,
    x_hbm,
    gain_hbm,
    ids_hbm,
    logits_hbm,
    gate_hbm,
    up_hbm,
    down_hbm,
    mixer_hbm,
    mix_out,
    routed_out,
    q_ref,
    k_ref,
    v_ref,
    x_ref,
    gain_ref,
    ids_ref,
    logits_ref,
    wg,
    wu,
    wd,
    wm,
    xs,
    xr,
    wr,
    kvr,
    pb,
    cr,
    sb,
    rr,
    zb,
    zr,
    at_send,
    at_recv,
    qt_ref,
    kv_ref,
    wt_ref,
    wc,
    acc,
    tot,
    hs,
    ob,
    ex,
    w_sem,
    in_sem,
    xf_ss,
    xf_rs,
    g_ss,
    g_rs,
    ff_ss,
    ff_rs,
    y_ss,
    y_rs,
    e_ss,
    e_rs,
    d_ss,
    cf_rs,
    d_rs,
    xn_ss,
    fn_ss,
    xn_rs,
    fn_rs,
    cn_rs,
    rn_rs,
    wt_rs,
    kv_ss,
    kv_rs,
    z_rs,
    a_rs,
    c0_rs,
    r_ss,
    c_ss,
    z_ss,
    a_ss,
    wt_ss,
    wave,
):
    e = lax.axis_index("ep")
    t = lax.axis_index("tp")
    core = t % 2
    zi = t // 2
    zs = n_tp // 2
    mate = t + 1 - 2 * core
    heads, seqs, seg, hd = qt_ref.shape
    tokens, width = x_ref.shape
    half = tokens // 2
    quarter = tokens // 4
    zp = zi % 2
    zmate = t + 2 - 4 * zp
    slots = wt_ref.shape[1]
    local_experts = wg.shape[0]
    ch = width // n_tp
    pp = seg // n_tp
    near, distances = split_sources(n_ep)
    passes = len(near)
    count = len(distances)
    part = tokens // passes
    upper, lower = pl.ds(0, half), pl.ds(half, half)
    everything = slice(None)

    weights = [
        pltpu.make_async_copy(src, dst, w_sem.at[i])
        for i, (src, dst) in enumerate(
            ((gate_hbm, wg), (up_hbm, wu), (down_hbm, wd), (mixer_hbm, wm))
        )
    ]
    inputs = [
        pltpu.make_async_copy(src, dst, in_sem.at[i])
        for i, (src, dst) in enumerate(
            (
                (x_hbm, x_ref),
                (q_hbm, q_ref),
                (k_hbm, k_ref),
                (v_hbm, v_ref),
                (ids_hbm, ids_ref),
                (logits_hbm, logits_ref),
                (gain_hbm, gain_ref),
            )
        )
    ]

    def ep_peer(d):
        return partner_of(e, d, n_ep)

    barrier = pltpu.get_barrier_semaphore()
    for d in range(1, n_ep):
        pl.semaphore_signal(barrier, inc=1, device_id={"ep": ep_peer(d)}, device_id_type=MESH)
    below, above = zi > 0, zi < zs - 1
    greeted = n_ep + below.astype(jnp.int32) + above.astype(jnp.int32)

    def signal(sem, to):
        pl.semaphore_signal(sem, inc=1, device_id={"tp": to}, device_id_type=MESH)

    signal(barrier, mate)

    @pl.when(below)
    def _():
        signal(barrier, t - 2)

    @pl.when(above)
    def _():
        signal(barrier, t + 2)

    def wave_start():
        @pl.when(jnp.logical_not(above))
        def _():
            signal(wave.at[0], t - 2)

        @pl.when(jnp.logical_not(below))
        def _():
            signal(wave.at[1], t + 2)

    def wave_pass(first):
        for way in range(2):
            turn = (zi < zs // 2) if first == (way == 1) else (zi >= zs // 2)

            @pl.when(below & above & turn)
            def _():
                pl.semaphore_wait(wave.at[way], 1)
                signal(wave.at[way], t + 4 * way - 2)

    def wave_end():
        @pl.when(jnp.logical_not(below))
        def _():
            pl.semaphore_wait(wave.at[0], 1)

        @pl.when(jnp.logical_not(above))
        def _():
            pl.semaphore_wait(wave.at[1], 1)

    for copy in inputs:
        copy.start()

    orders = [
        sorted((c for c in range(zs) if c != z), key=lambda c: -abs(c - z)) + [z]
        for z in range(zs)
    ]

    def chunk(k):
        return sum(jnp.where(zi == z, order[k - 1], 0) for z, order in enumerate(orders))

    def nth(i):
        return sum(jnp.where(i == n, d, 0) for n, d in enumerate(distances))

    def remote(src, dst, send, recv, axis, to):
        return pltpu.make_async_remote_copy(
            src_ref=src,
            dst_ref=dst,
            send_sem=send,
            recv_sem=recv,
            device_id={axis: to},
            device_id_type=MESH,
        )

    def settle_bytes(ref, sem):
        pltpu.make_async_copy(ref, ref, sem).wait()

    mine = pl.ds(pl.multiple_of(core * half, half), half)
    piece = pl.ds(pl.multiple_of(core * half + zp * quarter, quarter), quarter)

    def span(h):
        return pl.ds(pl.multiple_of(h * part, part), part)

    def own_part(h):
        return pl.ds(pl.multiple_of(h * part + core * (part // 2), part // 2), part // 2)

    def xf_copy(i):
        d = nth(i)
        return remote(xs.at[piece], xr.at[d, piece], xf_ss.at[i], xf_rs.at[i], "ep", ep_peer(d))

    def g_copy(i):
        ref = xr.at[nth(i), piece]
        return remote(ref, ref, g_ss.at[i], g_rs.at[i], "tp", zmate)

    def ff_copy(i):
        ref = xr.at[nth(i), mine]
        return remote(ref, ref, ff_ss.at[i], ff_rs.at[i], "tp", mate)

    def xn_copy(n, h):
        rows = own_part(h)
        return remote(
            xs.at[rows],
            xr.at[near[n], rows],
            xn_ss.at[n],
            xn_rs.at[n, h],
            "ep",
            ep_peer(near[n]),
        )

    def fn_copy(n, h):
        ref = xr.at[near[n], own_part(h)]
        return remote(ref, ref, fn_ss.at[n], fn_rs.at[n, h], "tp", mate)

    def wt_copy(d):
        return remote(
            wt_ref.at[ep_peer(d)], wr.at[d], wt_ss.at[0], wt_rs.at[d - 1], "ep", ep_peer(d)
        )

    def kv_copy(d):
        return remote(
            kv_ref, kvr.at[d], kv_ss.at[d - 1], kv_rs.at[d - 1], "ep", (e + d) % n_ep
        )

    def c_copy(d, c, rows, sem):
        return remote(
            pb.at[d, 1 - core, c, rows], cr.at[d, c, rows], c_ss.at[0], sem, "tp", mate
        )

    def r_copy(n, h, k):
        c = chunk(k)
        return remote(
            sb.at[near[n], c, span(h)],
            rr.at[near[n], c, span(h)],
            r_ss.at[0],
            rn_rs.at[h, k - 1],
            "ep",
            ep_peer(near[n]),
        )

    def y_copy(i, k):
        d = nth(i)
        c = chunk(k)
        return remote(
            sb.at[d, c, upper],
            rr.at[d, zi, upper],
            y_ss.at[i],
            y_rs.at[i],
            "tp",
            c * 2 + core,
        )

    def e_copy(i):
        d = nth(i)
        return remote(
            sb.at[d, zi, upper], ex.at[i], e_ss.at[i], e_rs.at[i], "ep", ep_peer(d)
        )

    def d_copy(i, k):
        d = nth(i)
        c = chunk(k)
        return remote(
            sb.at[d, c, lower],
            rr.at[d, c, lower],
            d_ss.at[i],
            d_rs.at[i, k - 1],
            "ep",
            ep_peer(d),
        )

    def z_copy(k, h):
        dz = chunk(k)
        return remote(
            zb.at[dz, span(h)],
            zr.at[zi, span(h)],
            z_ss.at[0],
            z_rs.at[0],
            "tp",
            dz * 2 + core,
        )

    def a_copy(d):
        to = (t + d) % n_tp
        return remote(at_send.at[to], at_recv.at[t], a_ss.at[0], a_rs.at[0], "tp", to)

    with scope("xload"):
        for copy in inputs:
            copy.wait()
    for copy in weights:
        copy.start()

    with scope("norm0"):
        values = x_ref[...].astype(f32)
        mean = jnp.mean(values * values, axis=-1, keepdims=True)
        xs[...] = (values * lax.rsqrt(mean + norm_eps) * gain_ref[...]).astype(bf16)

    top = ids_ref.shape[0]
    logits = [logits_ref[k : k + 1] for k in range(top)]
    peak = functools.reduce(jnp.maximum, logits)
    powers = [jnp.exp(value - peak) for value in logits]
    share = 1.0 / functools.reduce(jnp.add, powers)
    slot = lax.broadcasted_iota(jnp.int32, (slots, tokens), 0)
    for g in range(n_ep):
        expert = jnp.where(slot < local_experts, g * local_experts + slot, -1)
        table = jnp.zeros((slots, tokens), f32)
        for k in range(top):
            table = table + jnp.where(ids_ref[k : k + 1] == expert, powers[k] * share, 0.0)
        wt_ref[g] = table

    with scope("barrier"):
        pl.semaphore_wait(barrier, greeted)
    for d in range(1, n_ep):
        wt_copy(d).start()
    for i in range(count):
        xf_copy(i).start()
    for n in range(passes):
        xn_copy(n, 0).start()
    wave_start()

    rows = hd * seqs
    for s in range(seqs):
        pick = (
            (
                lax.broadcasted_iota(jnp.int32, (hd, rows), 1)
                == lax.broadcasted_iota(jnp.int32, (hd, rows), 0) * seqs + s
            )
            .astype(f32)
            .astype(bf16)
        )
        for h in range(heads):
            kv_ref[0, h, s] = jnp.dot(pick, k_ref[h], preferred_element_type=f32).astype(bf16)
            kv_ref[1, h, s] = jnp.dot(pick, v_ref[h], preferred_element_type=f32).astype(bf16)
            query = jnp.dot(pick, q_ref[h], preferred_element_type=f32)
            qt_ref[h, s] = query.T.astype(bf16)

    def up(j, lhs, columns):
        gate_pre = jnp.dot(lhs(), wg[j], preferred_element_type=f32)
        up_pre = jnp.dot(lhs(), wu[j], preferred_element_type=f32)
        hs[j] = activate(gate_pre, up_pre, columns[:, j : j + 1])

    def down(sources, rows, sem):
        size = tokens // len(sources)
        for k in range(1, zs + 1):
            c = chunk(k)
            for p in range(2):
                place = pl.ds(pl.multiple_of((2 * c + p) * ch, ch), ch)
                total = functools.reduce(
                    jnp.add,
                    [
                        jnp.dot(hs[j], wd[j, :, place], preferred_element_type=f32)
                        for j in range(local_experts)
                    ],
                ).astype(bf16)
                for n, d in enumerate(sources):
                    pb[d, p, c, rows] = total[n * size : (n + 1) * size]
        for k in range(1, zs + 1):
            for d in sources:
                c_copy(d, chunk(k), rows, sem).start()

    def joined(d, c, rows):
        sb[d, c, rows] = (pb[d, core, c, rows].astype(f32) + cr[d, c, rows].astype(f32)).astype(
            bf16
        )

    def finish_own():
        settle_bytes(cr.at[0], c0_rs.at[0])
        for c in range(zs):
            joined(0, c, everything)

    def finish_far(i):
        d = nth(i)
        settle_bytes(cr.at[d], cf_rs.at[i])
        for k in range(1, zs + 1):
            joined(d, chunk(k), everything)
            d_copy(i, k).start()
            if k < zs:
                y_copy(i, k).start()

    def finish_near(h):
        settle_bytes(cr.at[pl.ds(0, passes), :, span(h)], cn_rs.at[h])
        for k in range(1, zs + 1):
            for n in range(passes):
                joined(near[n], chunk(k), span(h))
                r_copy(n, h, k).start()

    def gathered(i):
        d = nth(i)
        settle_bytes(rr.at[d, pl.ds(0, zs - 1), upper], y_rs.at[i])
        total = sb[d, zi, upper].astype(f32)
        for k in range(1, zs):
            total = total + rr[d, chunk(k), upper].astype(f32)
        sb[d, zi, upper] = total.astype(bf16)
        e_copy(i).start()

    def settle(h):
        for k in range(1, zs + 1):
            c = chunk(k)
            own = sb[0, c, span(h)].astype(f32)
            settle_bytes(rr.at[pl.ds(0, passes), c, span(h)], rn_rs.at[h, k - 1])
            for n in range(passes):
                own = own + rr[near[n], c, span(h)].astype(f32)
            if h * part >= half:
                for i, d in enumerate(distances):
                    if h * part == half:
                        d_copy(i, k).wait_recv()
                    own = own + rr[d, c, span(h)].astype(f32)
            if k < zs:
                zb[c, span(h)] = own.astype(bf16)
                z_copy(k, h).start()
            else:
                ob[span(h)] = own

    pairs = heads * seqs
    tall = pairs * seg
    row_id = lax.broadcasted_iota(jnp.int32, (2 * seg, 2 * seg), 0) % seg
    col_id = lax.broadcasted_iota(jnp.int32, (2 * seg, 2 * seg), 1)
    later_mask = ((row_id > col_id) | (col_id >= seg)).astype(f32).astype(bf16)
    scale = hd ** (-0.5)

    def block(kv, diagonal):
        scores = jnp.concatenate(
            [
                jnp.dot(qt_ref[p // seqs, p % seqs], kv[0, p // seqs, p % seqs],
                        preferred_element_type=f32)
                for p in range(pairs)
            ],
            axis=0,
        ) * scale
        log_term = jnp.log(1.0 + jnp.exp(-jnp.abs(scores)))
        keep = -(jnp.maximum(scores, 0.0) + log_term)
        beta = jnp.minimum(scores, 0.0) - log_term
        if diagonal:
            usable = lax.broadcasted_iota(jnp.int32, (tall, seg), 1) < (
                lax.broadcasted_iota(jnp.int32, (tall, seg), 0) % seg
            )
            keep = jnp.where(usable, keep, 0.0)
        high = keep.astype(bf16)
        low = (keep - high.astype(f32)).astype(bf16)
        sums = jnp.dot(
            jnp.concatenate([high, low], axis=1), later_mask, preferred_element_type=f32
        )
        weight = jnp.exp(beta + sums[:, :seg])
        if diagonal:
            weight = jnp.where(usable, weight, 0.0)
        weight = weight.astype(bf16)
        out = jnp.concatenate(
            [
                lax.dot_general(
                    weight[p * seg : (p + 1) * seg],
                    kv[1, p // seqs, p % seqs],
                    (((1,), (1,)), ((), ())),
                    preferred_element_type=f32,
                )
                for p in range(pairs)
            ],
            axis=0,
        )
        return out, sums[:, seg : seg + hd]

    with scope("diag"):
        acc[...], tot[...] = block(kv_ref, True)

    def share_near(h):
        with scope("xwait"):
            for n in range(passes):
                xn_copy(n, h).wait_recv()
                fn_copy(n, h).start()

    def share_far(i):
        with scope("gwait"):
            g_copy(i).wait_recv()
            ff_copy(i).start()

    with scope("weights"):
        for copy in weights[:3]:
            copy.wait()
    own_columns = wt_ref[e].T
    with scope("up0"):
        up(0, lambda: xs[...], own_columns)
    with scope("waitfar"):
        for i in range(count):
            xf_copy(i).wait_recv()
            g_copy(i).start()
        for h in range(1, passes):
            for n in range(passes):
                xn_copy(n, h).start()
    with scope("up0"):
        for j in range(1, local_experts):
            up(j, lambda: xs[...], own_columns)
    share_near(0)
    with scope("down0"):
        down([0], everything, c0_rs.at[0])
    for k in range(1, n_ep):

        @pl.when(e + k < n_ep)
        def _():
            kv_copy(k).start()

    with scope("wave"):
        wave_pass(True)

    def near_pass(h, middle, spread=None):
        with scope("fwait"):
            for n in range(passes):
                fn_copy(n, h).wait_recv()

        def lhs():
            return jnp.concatenate([xr[d, span(h)] for d in near], axis=0)

        columns = jnp.concatenate([wc[n, span(h)] for n in range(passes)], axis=0)
        for j in range(local_experts):
            with scope("up"):
                up(j, lhs, columns)
            if j == 0 and spread is not None:
                spread()
        middle()
        with scope("down"):
            down(near, span(h), cn_rs.at[h])

    def far_pass(i, middle, spread):
        d = nth(i)
        with scope("fwait"):
            ff_copy(i).wait_recv()
            wt_copy(d).wait_recv()
        columns = wr[d].T
        for j in range(local_experts):
            with scope("up"):
                up(j, lambda: xr[d], columns)
            if j == 0:
                spread()
        middle()
        with scope("downfar"):
            down([d], everything, cf_rs.at[i])

    def first_passes(h, carry):
        @pl.when(h > 0)
        def _():
            share_near(h)

        def middle():
            with scope("finish"):

                @pl.when(h > 0)
                def _():
                    finish_near(h - 1)

                @pl.when(h == 0)
                def _():
                    finish_own()

        def spread():
            if distances:

                @pl.when(h == passes - 2)
                def _():
                    share_far(0)

        near_pass(h, middle, spread)
        return carry

    def far_passes(i, carry):
        def middle():
            @pl.when(i == 0)
            def _():
                with scope("finish"):
                    finish_near(passes - 2)

            @pl.when(i > 0)
            def _():
                finish_far(i - 1)

        def spread():
            @pl.when(i < count - 1)
            def _():
                share_far(i + 1)

            @pl.when(i == count - 1)
            def _():
                share_near(passes - 1)

        far_pass(i, middle, spread)
        return carry

    def last_middle():
        with scope("finishfar"):
            if distances:
                finish_far(count - 1)
            else:
                finish_own()

    def further(d, carry):
        kv_copy(d).wait_recv()
        out, total = block(kvr.at[d], False)
        later = tot[...]
        acc[...] = acc[...] + jnp.exp(later) * out
        tot[...] = later + total
        return carry

    def hand_out():
        with scope("asend"):
            for p in range(pairs):
                h, s = p // seqs, p % seqs
                for c in range(n_tp):
                    at_send[c, s * pp : (s + 1) * pp, h * hd : (h + 1) * hd] = acc[
                        p * seg + c * pp : p * seg + (c + 1) * pp
                    ].astype(bf16)
            for d in range(1, n_tp):
                a_copy(d).start()
            at_recv[t] = at_send[t]

    for n in range(passes):
        wt_copy(near[n]).wait_recv()
        wc[n] = wr[near[n]].T
    lax.fori_loop(0, passes - 1, first_passes, 0)
    with scope("wave"):
        wave_pass(False)
    lax.fori_loop(0, count, far_passes, 0)
    if not distances:
        share_near(passes - 1)
    with scope("wavend"):
        wave_end()
    early = n_ep // 2

    @pl.when(e == 0)
    def _():
        hand_out()

    near_pass(passes - 1, last_middle)
    with scope("further"):
        lax.fori_loop(1, jnp.minimum(e, early) + 1, further, 0)

    @pl.when((e > 0) & (e <= early))
    def _():
        hand_out()

    with scope("finlast"):
        finish_near(passes - 1)
    with scope("further"):
        lax.fori_loop(early + 1, e + 1, further, 0)

    @pl.when(e > early)
    def _():
        hand_out()


    for h in range(passes):
        if h == passes - 1:
            with scope("gathered"):
                lax.fori_loop(0, count, lambda i, carry: (gathered(i), carry)[1], 0)
        with scope("settle"):
            settle(h)

    with scope("wmix"):
        weights[3].wait()
    with scope("await"):
        settle_bytes(at_recv.at[pl.ds(0, n_tp - 1)], a_rs.at[0])
    with scope("mix"):
        wide = jnp.concatenate([at_recv[c] for c in range(n_tp)], axis=1)
        mixed = jnp.dot(wide, wm[...], preferred_element_type=f32)
        for s in range(seqs):
            mix_out[s] = mixed[s * pp : (s + 1) * pp].astype(bf16)

    with scope("zfin"):
        settle_bytes(zr.at[pl.ds(0, zs - 1)], z_rs.at[0])
        for i, d in enumerate(distances):
            e_copy(i).wait_recv()
            ob[upper] = ob[upper] + ex[i].astype(f32)
        total = ob[...]
        for k in range(1, zs):
            total = total + zr[chunk(k)].astype(f32)
        routed_out[...] = total.T.astype(bf16)

    with scope("drain"):
        settle_bytes(wt_ref.at[pl.ds(0, n_ep - 1)], wt_ss.at[0])
        for i in range(count):
            xf_copy(i).wait_send()
            g_copy(i).wait_send()
            ff_copy(i).wait_send()
            settle_bytes(sb.at[0, pl.ds(0, zs - 1), upper], y_ss.at[i])
            settle_bytes(sb.at[0, :, upper], d_ss.at[i])
            e_copy(i).wait_send()
        for n in range(passes):
            settle_bytes(xs.at[mine], xn_ss.at[n])
            settle_bytes(xs.at[mine], fn_ss.at[n])
        settle_bytes(cr, c_ss.at[0])
        settle_bytes(sb.at[pl.ds(0, passes)], r_ss.at[0])
        settle_bytes(zb.at[pl.ds(0, zs - 1)], z_ss.at[0])
        settle_bytes(at_send.at[pl.ds(0, n_tp - 1)], a_ss.at[0])
        for k in range(1, n_ep):

            @pl.when(e + k < n_ep)
            def _():
                kv_copy(k).wait_send()


def hand_over(mixed_ref, routed_ref, mix_out, routed_out, sems):
    copies = [
        pltpu.make_async_copy(src, dst, sems.at[i])
        for i, (src, dst) in enumerate(((mixed_ref, mix_out), (routed_ref, routed_out)))
    ]
    for copy in copies:
        copy.start()
    for copy in copies:
        copy.wait()


def body(
    queries,
    key_vectors,
    value_vectors,
    mixer_weight,
    expert_rows,
    norm_gain,
    route_ids,
    route_logits,
    gate_weight,
    up_weight,
    down_weight,
):
    n_ep, n_tp = lax.axis_size("ep"), lax.axis_size("tp")
    heads, hd, seqs, seg = queries.shape
    tokens, width = expert_rows.shape
    local_experts, _, ff = gate_weight.shape
    zs, ch, pp = n_tp // 2, width // n_tp, seg // n_tp

    top = route_ids.shape[1]
    slots = 8 * -(-local_experts // 8)
    pairs = heads * seqs
    near, distances = split_sources(n_ep)
    passes, count = len(near), max(len(distances), 1)
    kv_shape = (2, heads, seqs, hd, seg)

    def merged(rows):
        return rows.reshape(heads, hd * seqs, seg)

    vmem = pl.BlockSpec(memory_space=pltpu.VMEM)
    anywhere = pl.BlockSpec(memory_space=pltpu.HBM)
    dma = pltpu.SemaphoreType.DMA
    outs = 2 * seqs * pp * width + 2 * ch * tokens
    limit = (60 * 1024 * 1024) - outs - (64 << 10)
    shapes = ((seqs, pp, width), (ch, tokens))
    results = pl.pallas_call(
        functools.partial(kernel, n_ep, n_tp),
        out_shape=tuple(pltpu.VMEM(shape, bf16) for shape in shapes),
        in_specs=[anywhere] * 11,
        out_specs=(vmem, vmem),
        scratch_shapes=[
            pltpu.VMEM((heads, hd * seqs, seg), bf16),
            pltpu.VMEM((heads, hd * seqs, seg), bf16),
            pltpu.VMEM((heads, hd * seqs, seg), bf16),
            pltpu.VMEM((tokens, width), bf16),
            pltpu.VMEM((1, width), f32),
            pltpu.VMEM((top, tokens), jnp.int32),
            pltpu.VMEM((top, tokens), f32),
            pltpu.VMEM(gate_weight.shape, bf16),
            pltpu.VMEM(up_weight.shape, bf16),
            pltpu.VMEM(down_weight.shape, bf16),
            pltpu.VMEM(mixer_weight.shape, bf16),
            pltpu.VMEM((tokens, width), bf16),
            pltpu.VMEM((n_ep, tokens, width), bf16),
            pltpu.VMEM((n_ep, slots, tokens), f32),
            pltpu.VMEM((n_ep,) + kv_shape, bf16),
            pltpu.VMEM((n_ep, 2, zs, tokens, ch), bf16),
            pltpu.VMEM((n_ep, zs, tokens, ch), bf16),
            pltpu.VMEM((n_ep, zs, tokens, ch), bf16),
            pltpu.VMEM((n_ep, zs, tokens, ch), bf16),
            pltpu.VMEM((zs, tokens, ch), bf16),
            pltpu.VMEM((zs, tokens, ch), bf16),
            pltpu.VMEM((n_tp, seqs * pp, heads * hd), bf16),
            pltpu.VMEM((n_tp, seqs * pp, heads * hd), bf16),
            pltpu.VMEM((heads, seqs, seg, hd), bf16),
            pltpu.VMEM(kv_shape, bf16),
            pltpu.VMEM((n_ep, slots, tokens), f32),
            pltpu.VMEM((passes, tokens, slots), f32),
            pltpu.VMEM((pairs * seg, hd), f32),
            pltpu.VMEM((pairs * seg, hd), f32),
            pltpu.VMEM((local_experts, tokens, ff), bf16),
            pltpu.VMEM((tokens, ch), f32),
            pltpu.VMEM((count, tokens // 2, ch), bf16),
            dma((4,)),
            dma((7,)),
        ]
        + [dma((count,))] * 12
        + [dma((count, zs))]
        + [dma((passes,))] * 2
        + [dma((passes, passes))] * 2
        + [dma((passes,)), dma((passes, zs))]
        + [dma((n_ep - 1,))] * 3
        + [dma((1,))] * 8
        + [pltpu.SemaphoreType.REGULAR((2,))],
        compiler_params=pltpu.CompilerParams(
            collective_id=0, has_side_effects=True, vmem_limit_bytes=limit
        ),
    )(
        merged(queries),
        merged(key_vectors),
        merged(value_vectors),
        expert_rows,
        norm_gain[None, :],
        route_ids.T,
        route_logits.T,
        gate_weight,
        up_weight,
        down_weight,
        mixer_weight,
    )
    return pl.pallas_call(
        hand_over,
        out_shape=tuple(jax.ShapeDtypeStruct(shape, bf16) for shape in shapes),
        in_specs=[vmem] * 2,
        out_specs=(anywhere, anywhere),
        scratch_shapes=[dma((2,))],
        compiler_params=pltpu.CompilerParams(vmem_limit_bytes=1 << 20),
    )(*results)


def solution(mesh):
    in_specs = (
        P("tp", None, None, "ep"),
        P("tp", None, None, "ep"),
        P("tp", None, None, "ep"),
        P(),
        P("ep", None),
        P(),
        P("ep", None),
        P("ep", None),
        P("ep", None, "tp"),
        P("ep", None, "tp"),
        P("ep", "tp", None),
    )
    out_specs = (P(None, ("ep", "tp"), None), P("tp", "ep"))
    return jax.shard_map(body, mesh=mesh, in_specs=in_specs, out_specs=out_specs, check_vma=False)
```

```python
import functools

import jax
import jax.numpy as jnp
from jax import lax
from jax.experimental import pallas as pl
from jax.experimental.pallas import tpu as pltpu
from jax.sharding import PartitionSpec as P

limit_value = 7.0
alpha_value = 1.702
norm_eps = 1e-06

MESH = pl.DeviceIdType.MESH
f32 = jnp.float32
bf16 = jnp.bfloat16
scope = jax.named_scope


def activate(gate_pre, up_pre, weight):
    g = jnp.minimum(gate_pre, limit_value)
    u = jnp.clip(up_pre, -limit_value, limit_value)
    sigmoid2 = 1.0 + jnp.tanh((0.5 * alpha_value) * g)
    return ((u + 1.0) * (g * (0.5 * weight)) * sigmoid2).astype(bf16)


def partner_of(me, offset, count):
    other = me
    bit = 1
    while bit < count:
        set_bit = (offset // bit) % 2
        other = other + set_bit * bit * (1 - 2 * ((me // bit) % 2))
        bit *= 2
    return other


def split_sources(n_ep):
    near = [d for d in range(1, n_ep) if d & (d - 1) == 0][::-1]
    far = [d for d in range(1, n_ep) if d & (d - 1) != 0][::-1]
    return near, far


def kernel(
    n_ep,
    n_tp,
    q_hbm,
    k_hbm,
    v_hbm,
    x_hbm,
    gain_hbm,
    ids_hbm,
    logits_hbm,
    gate_hbm,
    up_hbm,
    down_hbm,
    mixer_hbm,
    mix_out,
    routed_out,
    q_ref,
    k_ref,
    v_ref,
    x_ref,
    gain_ref,
    ids_ref,
    logits_ref,
    wg,
    wu,
    wd,
    wm,
    xs,
    xr,
    wr,
    kvr,
    pb,
    cr,
    sb,
    rr,
    zb,
    zr,
    at_send,
    at_recv,
    qt_ref,
    kv_ref,
    wt_ref,
    wc,
    acc,
    tot,
    hs,
    ob,
    ex,
    w_sem,
    in_sem,
    xf_ss,
    xf_rs,
    g_ss,
    g_rs,
    ff_ss,
    ff_rs,
    y_ss,
    y_rs,
    e_ss,
    e_rs,
    d_ss,
    cf_rs,
    d_rs,
    xn_ss,
    fn_ss,
    xn_rs,
    fn_rs,
    cn_rs,
    rn_rs,
    wt_rs,
    kv_ss,
    kv_rs,
    z_rs,
    a_rs,
    c0_rs,
    r_ss,
    c_ss,
    z_ss,
    a_ss,
    wt_ss,
    wave,
):
    e = lax.axis_index("ep")
    t = lax.axis_index("tp")
    core = t % 2
    zi = t // 2
    zs = n_tp // 2
    mate = t + 1 - 2 * core
    heads, seqs, seg, hd = qt_ref.shape
    tokens, width = x_ref.shape
    half = tokens // 2
    quarter = tokens // 4
    zp = zi % 2
    zmate = t + 2 - 4 * zp
    slots = wt_ref.shape[1]
    local_experts = wg.shape[0]
    ch = width // n_tp
    pp = seg // n_tp
    near, distances = split_sources(n_ep)
    passes = len(near)
    count = len(distances)
    part = tokens // passes
    upper, lower = pl.ds(0, half), pl.ds(half, half)
    everything = slice(None)

    weights = [
        pltpu.make_async_copy(src, dst, w_sem.at[i])
        for i, (src, dst) in enumerate(
            ((gate_hbm, wg), (up_hbm, wu), (down_hbm, wd), (mixer_hbm, wm))
        )
    ]
    inputs = [
        pltpu.make_async_copy(src, dst, in_sem.at[i])
        for i, (src, dst) in enumerate(
            (
                (x_hbm, x_ref),
                (q_hbm, q_ref),
                (k_hbm, k_ref),
                (v_hbm, v_ref),
                (ids_hbm, ids_ref),
                (logits_hbm, logits_ref),
                (gain_hbm, gain_ref),
            )
        )
    ]

    def ep_peer(d):
        return partner_of(e, d, n_ep)

    barrier = pltpu.get_barrier_semaphore()
    for d in range(1, n_ep):
        pl.semaphore_signal(barrier, inc=1, device_id={"ep": ep_peer(d)}, device_id_type=MESH)
    below, above = zi > 0, zi < zs - 1
    greeted = n_ep + below.astype(jnp.int32) + above.astype(jnp.int32)

    def signal(sem, to):
        pl.semaphore_signal(sem, inc=1, device_id={"tp": to}, device_id_type=MESH)

    signal(barrier, mate)

    @pl.when(below)
    def _():
        signal(barrier, t - 2)

    @pl.when(above)
    def _():
        signal(barrier, t + 2)

    def wave_start():
        @pl.when(jnp.logical_not(above))
        def _():
            signal(wave.at[0], t - 2)

        @pl.when(jnp.logical_not(below))
        def _():
            signal(wave.at[1], t + 2)

    def wave_pass(first):
        for way in range(2):
            turn = (zi < zs // 2) if first == (way == 1) else (zi >= zs // 2)

            @pl.when(below & above & turn)
            def _():
                pl.semaphore_wait(wave.at[way], 1)
                signal(wave.at[way], t + 4 * way - 2)

    def wave_end():
        @pl.when(jnp.logical_not(below))
        def _():
            pl.semaphore_wait(wave.at[0], 1)

        @pl.when(jnp.logical_not(above))
        def _():
            pl.semaphore_wait(wave.at[1], 1)

    for copy in inputs:
        copy.start()

    orders = [
        sorted((c for c in range(zs) if c != z), key=lambda c: -abs(c - z)) + [z]
        for z in range(zs)
    ]

    def chunk(k):
        return sum(jnp.where(zi == z, order[k - 1], 0) for z, order in enumerate(orders))

    def nth(i):
        return sum(jnp.where(i == n, d, 0) for n, d in enumerate(distances))

    def remote(src, dst, send, recv, axis, to):
        return pltpu.make_async_remote_copy(
            src_ref=src,
            dst_ref=dst,
            send_sem=send,
            recv_sem=recv,
            device_id={axis: to},
            device_id_type=MESH,
        )

    def settle_bytes(ref, sem):
        pltpu.make_async_copy(ref, ref, sem).wait()

    mine = pl.ds(pl.multiple_of(core * half, half), half)
    piece = pl.ds(pl.multiple_of(core * half + zp * quarter, quarter), quarter)

    def span(h):
        return pl.ds(pl.multiple_of(h * part, part), part)

    def own_part(h):
        return pl.ds(pl.multiple_of(h * part + core * (part // 2), part // 2), part // 2)

    def xf_copy(i):
        d = nth(i)
        return remote(xs.at[piece], xr.at[d, piece], xf_ss.at[i], xf_rs.at[i], "ep", ep_peer(d))

    def g_copy(i):
        ref = xr.at[nth(i), piece]
        return remote(ref, ref, g_ss.at[i], g_rs.at[i], "tp", zmate)

    def ff_copy(i):
        ref = xr.at[nth(i), mine]
        return remote(ref, ref, ff_ss.at[i], ff_rs.at[i], "tp", mate)

    def xn_copy(n, h):
        rows = own_part(h)
        return remote(
            xs.at[rows],
            xr.at[near[n], rows],
            xn_ss.at[n],
            xn_rs.at[n, h],
            "ep",
            ep_peer(near[n]),
        )

    def fn_copy(n, h):
        ref = xr.at[near[n], own_part(h)]
        return remote(ref, ref, fn_ss.at[n], fn_rs.at[n, h], "tp", mate)

    def wt_copy(d):
        return remote(
            wt_ref.at[ep_peer(d)], wr.at[d], wt_ss.at[0], wt_rs.at[d - 1], "ep", ep_peer(d)
        )

    def kv_copy(d):
        return remote(
            kv_ref, kvr.at[d], kv_ss.at[d - 1], kv_rs.at[d - 1], "ep", (e + d) % n_ep
        )

    def c_copy(d, c, rows, sem):
        return remote(
            pb.at[d, 1 - core, c, rows], cr.at[d, c, rows], c_ss.at[0], sem, "tp", mate
        )

    def r_copy(n, h, k):
        c = chunk(k)
        return remote(
            sb.at[near[n], c, span(h)],
            rr.at[near[n], c, span(h)],
            r_ss.at[0],
            rn_rs.at[h, k - 1],
            "ep",
            ep_peer(near[n]),
        )

    def y_copy(i, k):
        d = nth(i)
        c = chunk(k)
        return remote(
            sb.at[d, c, upper],
            rr.at[d, zi, upper],
            y_ss.at[i],
            y_rs.at[i],
            "tp",
            c * 2 + core,
        )

    def e_copy(i):
        d = nth(i)
        return remote(
            sb.at[d, zi, upper], ex.at[i], e_ss.at[i], e_rs.at[i], "ep", ep_peer(d)
        )

    def d_copy(i, k):
        d = nth(i)
        c = chunk(k)
        return remote(
            sb.at[d, c, lower],
            rr.at[d, c, lower],
            d_ss.at[i],
            d_rs.at[i, k - 1],
            "ep",
            ep_peer(d),
        )

    def z_copy(k, h):
        dz = chunk(k)
        return remote(
            zb.at[dz, span(h)],
            zr.at[zi, span(h)],
            z_ss.at[0],
            z_rs.at[0],
            "tp",
            dz * 2 + core,
        )

    def a_copy(d):
        to = (t + d) % n_tp
        return remote(at_send.at[to], at_recv.at[t], a_ss.at[0], a_rs.at[0], "tp", to)

    with scope("xload"):
        for copy in inputs:
            copy.wait()
    for copy in weights:
        copy.start()

    with scope("norm0"):
        values = x_ref[...].astype(f32)
        mean = jnp.mean(values * values, axis=-1, keepdims=True)
        xs[...] = (values * lax.rsqrt(mean + norm_eps) * gain_ref[...]).astype(bf16)

    top = ids_ref.shape[0]
    logits = [logits_ref[k : k + 1] for k in range(top)]
    peak = functools.reduce(jnp.maximum, logits)
    powers = [jnp.exp(value - peak) for value in logits]
    share = 1.0 / functools.reduce(jnp.add, powers)
    slot = lax.broadcasted_iota(jnp.int32, (slots, tokens), 0)
    for g in range(n_ep):
        expert = jnp.where(slot < local_experts, g * local_experts + slot, -1)
        table = jnp.zeros((slots, tokens), f32)
        for k in range(top):
            table = table + jnp.where(ids_ref[k : k + 1] == expert, powers[k] * share, 0.0)
        wt_ref[g] = table

    with scope("barrier"):
        pl.semaphore_wait(barrier, greeted)
    for d in range(1, n_ep):
        wt_copy(d).start()
    for i in range(count):
        xf_copy(i).start()
    for n in range(passes):
        xn_copy(n, 0).start()
    wave_start()

    rows = hd * seqs
    for s in range(seqs):
        pick = (
            (
                lax.broadcasted_iota(jnp.int32, (hd, rows), 1)
                == lax.broadcasted_iota(jnp.int32, (hd, rows), 0) * seqs + s
            )
            .astype(f32)
            .astype(bf16)
        )
        for h in range(heads):
            kv_ref[0, h, s] = jnp.dot(pick, k_ref[h], preferred_element_type=f32).astype(bf16)
            kv_ref[1, h, s] = jnp.dot(pick, v_ref[h], preferred_element_type=f32).astype(bf16)
            query = jnp.dot(pick, q_ref[h], preferred_element_type=f32)
            qt_ref[h, s] = query.T.astype(bf16)

    def up(j, lhs, columns):
        gate_pre = jnp.dot(lhs(), wg[j], preferred_element_type=f32)
        up_pre = jnp.dot(lhs(), wu[j], preferred_element_type=f32)
        hs[j] = activate(gate_pre, up_pre, columns[:, j : j + 1])

    def down(sources, rows, sem):
        size = tokens // len(sources)
        for k in range(1, zs + 1):
            c = chunk(k)
            for p in range(2):
                place = pl.ds(pl.multiple_of((2 * c + p) * ch, ch), ch)
                total = functools.reduce(
                    jnp.add,
                    [
                        jnp.dot(hs[j], wd[j, :, place], preferred_element_type=f32)
                        for j in range(local_experts)
                    ],
                ).astype(bf16)
                for n, d in enumerate(sources):
                    pb[d, p, c, rows] = total[n * size : (n + 1) * size]
        for k in range(1, zs + 1):
            for d in sources:
                c_copy(d, chunk(k), rows, sem).start()

    def joined(d, c, rows):
        sb[d, c, rows] = (pb[d, core, c, rows].astype(f32) + cr[d, c, rows].astype(f32)).astype(
            bf16
        )

    def finish_own():
        settle_bytes(cr.at[0], c0_rs.at[0])
        for c in range(zs):
            joined(0, c, everything)

    def finish_far(i):
        d = nth(i)
        settle_bytes(cr.at[d], cf_rs.at[i])
        for k in range(1, zs + 1):
            joined(d, chunk(k), everything)
            d_copy(i, k).start()
            if k < zs:
                y_copy(i, k).start()

    def finish_near(h):
        settle_bytes(cr.at[pl.ds(0, passes), :, span(h)], cn_rs.at[h])
        for k in range(1, zs + 1):
            for n in range(passes):
                joined(near[n], chunk(k), span(h))
                r_copy(n, h, k).start()

    def gathered(i):
        d = nth(i)
        settle_bytes(rr.at[d, pl.ds(0, zs - 1), upper], y_rs.at[i])
        total = sb[d, zi, upper].astype(f32)
        for k in range(1, zs):
            total = total + rr[d, chunk(k), upper].astype(f32)
        sb[d, zi, upper] = total.astype(bf16)
        e_copy(i).start()

    def settle(h):
        for k in range(1, zs + 1):
            c = chunk(k)
            own = sb[0, c, span(h)].astype(f32)
            settle_bytes(rr.at[pl.ds(0, passes), c, span(h)], rn_rs.at[h, k - 1])
            for n in range(passes):
                own = own + rr[near[n], c, span(h)].astype(f32)
            if h * part >= half:
                for i, d in enumerate(distances):
                    if h * part == half:
                        d_copy(i, k).wait_recv()
                    own = own + rr[d, c, span(h)].astype(f32)
            if k < zs:
                zb[c, span(h)] = own.astype(bf16)
                z_copy(k, h).start()
            else:
                ob[span(h)] = own

    pairs = heads * seqs
    tall = pairs * seg
    row_id = lax.broadcasted_iota(jnp.int32, (2 * seg, 2 * seg), 0) % seg
    col_id = lax.broadcasted_iota(jnp.int32, (2 * seg, 2 * seg), 1)
    later_mask = ((row_id > col_id) | (col_id >= seg)).astype(f32).astype(bf16)
    scale = hd ** (-0.5)

    def block(kv, diagonal):
        scores = jnp.concatenate(
            [
                jnp.dot(qt_ref[p // seqs, p % seqs], kv[0, p // seqs, p % seqs],
                        preferred_element_type=f32)
                for p in range(pairs)
            ],
            axis=0,
        ) * scale
        log_term = jnp.log(1.0 + jnp.exp(-jnp.abs(scores)))
        keep = -(jnp.maximum(scores, 0.0) + log_term)
        beta = jnp.minimum(scores, 0.0) - log_term
        if diagonal:
            usable = lax.broadcasted_iota(jnp.int32, (tall, seg), 1) < (
                lax.broadcasted_iota(jnp.int32, (tall, seg), 0) % seg
            )
            keep = jnp.where(usable, keep, 0.0)
        high = keep.astype(bf16)
        low = (keep - high.astype(f32)).astype(bf16)
        sums = jnp.dot(
            jnp.concatenate([high, low], axis=1), later_mask, preferred_element_type=f32
        )
        weight = jnp.exp(beta + sums[:, :seg])
        if diagonal:
            weight = jnp.where(usable, weight, 0.0)
        weight = weight.astype(bf16)
        out = jnp.concatenate(
            [
                lax.dot_general(
                    weight[p * seg : (p + 1) * seg],
                    kv[1, p // seqs, p % seqs],
                    (((1,), (1,)), ((), ())),
                    preferred_element_type=f32,
                )
                for p in range(pairs)
            ],
            axis=0,
        )
        return out, sums[:, seg : seg + hd]

    with scope("diag"):
        acc[...], tot[...] = block(kv_ref, True)

    def share_near(h):
        with scope("xwait"):
            for n in range(passes):
                xn_copy(n, h).wait_recv()
                fn_copy(n, h).start()

    def share_far(i):
        with scope("gwait"):
            g_copy(i).wait_recv()
            ff_copy(i).start()

    with scope("weights"):
        for copy in weights[:3]:
            copy.wait()
    own_columns = wt_ref[e].T
    with scope("up0"):
        up(0, lambda: xs[...], own_columns)
    with scope("waitfar"):
        for i in range(count):
            xf_copy(i).wait_recv()
            g_copy(i).start()
        for h in range(1, passes):
            for n in range(passes):
                xn_copy(n, h).start()
    with scope("up0"):
        for j in range(1, local_experts):
            up(j, lambda: xs[...], own_columns)
    share_near(0)
    with scope("down0"):
        down([0], everything, c0_rs.at[0])
    with scope("wave"):
        wave_pass(True)

    def near_pass(h, middle, spread=None):
        with scope("fwait"):
            for n in range(passes):
                fn_copy(n, h).wait_recv()

        def lhs():
            return jnp.concatenate([xr[d, span(h)] for d in near], axis=0)

        columns = jnp.concatenate([wc[n, span(h)] for n in range(passes)], axis=0)
        for j in range(local_experts):
            with scope("up"):
                up(j, lhs, columns)
            if j == 0 and spread is not None:
                spread()
        middle()
        with scope("down"):
            down(near, span(h), cn_rs.at[h])

    def far_pass(i, middle, spread):
        d = nth(i)
        with scope("fwait"):
            ff_copy(i).wait_recv()
            wt_copy(d).wait_recv()
        columns = wr[d].T
        for j in range(local_experts):
            with scope("up"):
                up(j, lambda: xr[d], columns)
            if j == 0:
                spread()
        middle()
        with scope("downfar"):
            down([d], everything, cf_rs.at[i])

    def send_kv(later):
        for k in range(1, n_ep):
            held = (e % 4 == 0) & (k % 4 < 3)

            @pl.when((e + k < n_ep) & (held == later))
            def _():
                kv_copy(k).start()

    send_kv(False)

    def first_passes(h, carry):
        @pl.when(h > 0)
        def _():
            share_near(h)

        def middle():
            with scope("finish"):

                @pl.when(h > 0)
                def _():
                    finish_near(h - 1)

                @pl.when(h == 0)
                def _():
                    finish_own()

        def spread():
            if distances:

                @pl.when(h == passes - 2)
                def _():
                    share_far(0)

            @pl.when(h == 0)
            def _():
                send_kv(True)

        near_pass(h, middle, spread)
        return carry

    def far_passes(i, carry):
        def middle():
            @pl.when(i == 0)
            def _():
                with scope("finish"):
                    finish_near(passes - 2)

            @pl.when(i > 0)
            def _():
                finish_far(i - 1)

        def spread():
            @pl.when(i < count - 1)
            def _():
                share_far(i + 1)

            @pl.when(i == count - 1)
            def _():
                share_near(passes - 1)

        far_pass(i, middle, spread)
        return carry

    def last_middle():
        with scope("finishfar"):
            if distances:
                finish_far(count - 1)
            else:
                finish_own()

    def further(d, carry):
        kv_copy(d).wait_recv()
        out, total = block(kvr.at[d], False)
        later = tot[...]
        acc[...] = acc[...] + jnp.exp(later) * out
        tot[...] = later + total
        return carry

    def hand_out():
        with scope("asend"):
            for p in range(pairs):
                h, s = p // seqs, p % seqs
                for c in range(n_tp):
                    at_send[c, s * pp : (s + 1) * pp, h * hd : (h + 1) * hd] = acc[
                        p * seg + c * pp : p * seg + (c + 1) * pp
                    ].astype(bf16)
            for d in range(1, n_tp):
                a_copy(d).start()
            at_recv[t] = at_send[t]

    for n in range(passes):
        wt_copy(near[n]).wait_recv()
        wc[n] = wr[near[n]].T
    lax.fori_loop(0, passes - 1, first_passes, 0)
    with scope("wave"):
        wave_pass(False)
    lax.fori_loop(0, count, far_passes, 0)
    if not distances:
        share_near(passes - 1)
    with scope("wavend"):
        wave_end()
    early = n_ep // 2

    @pl.when(e == 0)
    def _():
        hand_out()

    near_pass(passes - 1, last_middle)
    with scope("further"):
        lax.fori_loop(1, jnp.minimum(e, early) + 1, further, 0)

    @pl.when((e > 0) & (e <= early))
    def _():
        hand_out()

    with scope("finlast"):
        finish_near(passes - 1)
    with scope("further"):
        lax.fori_loop(early + 1, e + 1, further, 0)

    @pl.when(e > early)
    def _():
        hand_out()


    for h in range(passes):
        if h == passes - 1:
            with scope("gathered"):
                lax.fori_loop(0, count, lambda i, carry: (gathered(i), carry)[1], 0)
        with scope("settle"):
            settle(h)

    with scope("wmix"):
        weights[3].wait()
    with scope("await"):
        settle_bytes(at_recv.at[pl.ds(0, n_tp - 1)], a_rs.at[0])
    with scope("mix"):
        wide = jnp.concatenate([at_recv[c] for c in range(n_tp)], axis=1)
        mixed = jnp.dot(wide, wm[...], preferred_element_type=f32)
        for s in range(seqs):
            mix_out[s] = mixed[s * pp : (s + 1) * pp].astype(bf16)

    with scope("zfin"):
        settle_bytes(zr.at[pl.ds(0, zs - 1)], z_rs.at[0])
        for i, d in enumerate(distances):
            e_copy(i).wait_recv()
            ob[upper] = ob[upper] + ex[i].astype(f32)
        total = ob[...]
        for k in range(1, zs):
            total = total + zr[chunk(k)].astype(f32)
        routed_out[...] = total.T.astype(bf16)

    with scope("drain"):
        settle_bytes(wt_ref.at[pl.ds(0, n_ep - 1)], wt_ss.at[0])
        for i in range(count):
            xf_copy(i).wait_send()
            g_copy(i).wait_send()
            ff_copy(i).wait_send()
            settle_bytes(sb.at[0, pl.ds(0, zs - 1), upper], y_ss.at[i])
            settle_bytes(sb.at[0, :, upper], d_ss.at[i])
            e_copy(i).wait_send()
        for n in range(passes):
            settle_bytes(xs.at[mine], xn_ss.at[n])
            settle_bytes(xs.at[mine], fn_ss.at[n])
        settle_bytes(cr, c_ss.at[0])
        settle_bytes(sb.at[pl.ds(0, passes)], r_ss.at[0])
        settle_bytes(zb.at[pl.ds(0, zs - 1)], z_ss.at[0])
        settle_bytes(at_send.at[pl.ds(0, n_tp - 1)], a_ss.at[0])
        for k in range(1, n_ep):

            @pl.when(e + k < n_ep)
            def _():
                kv_copy(k).wait_send()


def hand_over(mixed_ref, routed_ref, mix_out, routed_out, sems):
    copies = [
        pltpu.make_async_copy(src, dst, sems.at[i])
        for i, (src, dst) in enumerate(((mixed_ref, mix_out), (routed_ref, routed_out)))
    ]
    for copy in copies:
        copy.start()
    for copy in copies:
        copy.wait()


def body(
    queries,
    key_vectors,
    value_vectors,
    mixer_weight,
    expert_rows,
    norm_gain,
    route_ids,
    route_logits,
    gate_weight,
    up_weight,
    down_weight,
):
    n_ep, n_tp = lax.axis_size("ep"), lax.axis_size("tp")
    heads, hd, seqs, seg = queries.shape
    tokens, width = expert_rows.shape
    local_experts, _, ff = gate_weight.shape
    zs, ch, pp = n_tp // 2, width // n_tp, seg // n_tp

    top = route_ids.shape[1]
    slots = 8 * -(-local_experts // 8)
    pairs = heads * seqs
    near, distances = split_sources(n_ep)
    passes, count = len(near), max(len(distances), 1)
    kv_shape = (2, heads, seqs, hd, seg)

    def merged(rows):
        return rows.reshape(heads, hd * seqs, seg)

    vmem = pl.BlockSpec(memory_space=pltpu.VMEM)
    anywhere = pl.BlockSpec(memory_space=pltpu.HBM)
    dma = pltpu.SemaphoreType.DMA
    outs = 2 * seqs * pp * width + 2 * ch * tokens
    limit = (60 * 1024 * 1024) - outs - (64 << 10)
    shapes = ((seqs, pp, width), (ch, tokens))
    results = pl.pallas_call(
        functools.partial(kernel, n_ep, n_tp),
        out_shape=tuple(pltpu.VMEM(shape, bf16) for shape in shapes),
        in_specs=[anywhere] * 11,
        out_specs=(vmem, vmem),
        scratch_shapes=[
            pltpu.VMEM((heads, hd * seqs, seg), bf16),
            pltpu.VMEM((heads, hd * seqs, seg), bf16),
            pltpu.VMEM((heads, hd * seqs, seg), bf16),
            pltpu.VMEM((tokens, width), bf16),
            pltpu.VMEM((1, width), f32),
            pltpu.VMEM((top, tokens), jnp.int32),
            pltpu.VMEM((top, tokens), f32),
            pltpu.VMEM(gate_weight.shape, bf16),
            pltpu.VMEM(up_weight.shape, bf16),
            pltpu.VMEM(down_weight.shape, bf16),
            pltpu.VMEM(mixer_weight.shape, bf16),
            pltpu.VMEM((tokens, width), bf16),
            pltpu.VMEM((n_ep, tokens, width), bf16),
            pltpu.VMEM((n_ep, slots, tokens), f32),
            pltpu.VMEM((n_ep,) + kv_shape, bf16),
            pltpu.VMEM((n_ep, 2, zs, tokens, ch), bf16),
            pltpu.VMEM((n_ep, zs, tokens, ch), bf16),
            pltpu.VMEM((n_ep, zs, tokens, ch), bf16),
            pltpu.VMEM((n_ep, zs, tokens, ch), bf16),
            pltpu.VMEM((zs, tokens, ch), bf16),
            pltpu.VMEM((zs, tokens, ch), bf16),
            pltpu.VMEM((n_tp, seqs * pp, heads * hd), bf16),
            pltpu.VMEM((n_tp, seqs * pp, heads * hd), bf16),
            pltpu.VMEM((heads, seqs, seg, hd), bf16),
            pltpu.VMEM(kv_shape, bf16),
            pltpu.VMEM((n_ep, slots, tokens), f32),
            pltpu.VMEM((passes, tokens, slots), f32),
            pltpu.VMEM((pairs * seg, hd), f32),
            pltpu.VMEM((pairs * seg, hd), f32),
            pltpu.VMEM((local_experts, tokens, ff), bf16),
            pltpu.VMEM((tokens, ch), f32),
            pltpu.VMEM((count, tokens // 2, ch), bf16),
            dma((4,)),
            dma((7,)),
        ]
        + [dma((count,))] * 12
        + [dma((count, zs))]
        + [dma((passes,))] * 2
        + [dma((passes, passes))] * 2
        + [dma((passes,)), dma((passes, zs))]
        + [dma((n_ep - 1,))] * 3
        + [dma((1,))] * 8
        + [pltpu.SemaphoreType.REGULAR((2,))],
        compiler_params=pltpu.CompilerParams(
            collective_id=0, has_side_effects=True, vmem_limit_bytes=limit
        ),
    )(
        merged(queries),
        merged(key_vectors),
        merged(value_vectors),
        expert_rows,
        norm_gain[None, :],
        route_ids.T,
        route_logits.T,
        gate_weight,
        up_weight,
        down_weight,
        mixer_weight,
    )
    return pl.pallas_call(
        hand_over,
        out_shape=tuple(jax.ShapeDtypeStruct(shape, bf16) for shape in shapes),
        in_specs=[vmem] * 2,
        out_specs=(anywhere, anywhere),
        scratch_shapes=[dma((2,))],
        compiler_params=pltpu.CompilerParams(vmem_limit_bytes=1 << 20),
    )(*results)


def solution(mesh):
    in_specs = (
        P("tp", None, None, "ep"),
        P("tp", None, None, "ep"),
        P("tp", None, None, "ep"),
        P(),
        P("ep", None),
        P(),
        P("ep", None),
        P("ep", None),
        P("ep", None, "tp"),
        P("ep", None, "tp"),
        P("ep", "tp", None),
    )
    out_specs = (P(None, ("ep", "tp"), None), P("tp", "ep"))
    return jax.shard_map(body, mesh=mesh, in_specs=in_specs, out_specs=out_specs, check_vma=False)
```
